512 devices in a mesh: sp: 64 (over z, y), tp: 8 (over x, core).
Axes of the slice: x: 4, y: 4, z: 16, core: 2. Of those that a mesh axis runs over, the one named last changes fastest.
Arguments:
- inputs: bfloat16 [16384, 4096], P('sp', 'tp'), may hold values from -20 to 20
- norm_gain: float32 [3, 4096], replicated, may hold values from 0.1 to 1.9
- in_weight: bfloat16 [3, 4096, 1024], P(None, 'tp', 'sp'), may hold values from -0.09375 to 0.09375
- pool_scale: float32 [3, 1024], replicated, may hold values from 0.1 to 1.9
- out_weight: bfloat16 [3, 1024, 4096], P(None, 'sp', 'tp'), may hold values from -0.1875 to 0.1875
Outputs:
- final_state: bfloat16 [16384, 4096], P('sp', 'tp')
The draws below stay inside these ranges and needn't reach their ends.
All inputs are finite; a program needn't handle non-finite values.
Results may differ from the reference program's by a relative error of at most 0.017.
Values may be sent and summed in bfloat16 or wider, within the bound.
A program may use at most 64 MiB of HBM per device.

```python
import jax
import jax.numpy as jnp
from jax import lax

D = 4096
P_SIZE = 1024
LAYERS = 3
TOKENS = 16384


def draw_inputs(key, part):
    column = lax.broadcasted_iota(jnp.float32, (1, D), 1) / D
    rough = jax.random.uniform(jax.random.fold_in(key, 2), (1, D), jnp.float32, 0.6, 1.4)
    column_scale = 0.35 * jnp.exp(jnp.log(10.0) * column) * rough
    base = jnp.clip(jax.random.normal(jax.random.fold_in(key, 1), (TOKENS, D), jnp.float32), -4.0, 4.0)
    return jnp.clip(base * column_scale, -20.0, 20.0).astype(jnp.bfloat16)


def levels(own_key, shape, split, least, largest):
    level = 1.0
    for dim, shards_of in split:
        heights = jax.random.uniform(jax.random.fold_in(jax.random.fold_in(own_key, 6), dim), (shards_of,), jnp.float32, least / len(split), largest / len(split))
        level = level * jnp.repeat(jnp.exp(heights), shape[dim] // shards_of).reshape((-1,) + (1,) * (len(shape) - 1 - dim))
    return level


def centred(own_key, extent, deviation, reach, pieces=(), dtype=jnp.bfloat16):
    values = jax.random.normal(own_key, extent, jnp.float32) * deviation
    if len(pieces) > 0:
        values = levels(own_key, extent, pieces, -0.22, 0.18) * values
    return jnp.clip(values, min=-reach, max=reach).astype(dtype)


def setup_inputs(seed: int = 0) -> dict:
    keys = jax.random.split(jax.random.key(seed), 6)
    inputs = draw_inputs(jax.random.fold_in(keys[5], 71), 0)
    norm_gain = jnp.clip(1.0 + 0.18 * jax.random.normal(keys[1], (LAYERS, D), jnp.float32), 0.1, 1.9)
    in_weight = centred(keys[2], (LAYERS, D, P_SIZE), D ** -0.5, 0.09375, ((1, 8), (2, 64)))
    pool_scale = jnp.clip(1.0 + 0.18 * jax.random.normal(keys[3], (LAYERS, P_SIZE), jnp.float32), 0.1, 1.9)
    out_weight = centred(keys[4], (LAYERS, P_SIZE, D), P_SIZE ** -0.5, 0.1875, ((1, 64), (2, 8)))
    return {"inputs": inputs, "norm_gain": norm_gain, "in_weight": in_weight, "pool_scale": pool_scale, "out_weight": out_weight}


epsilon = 1e-06
halo_rows = 16
group_count = 4

def window_means(extended, row_count, first_channel, first_pos, pool_total):
    width = extended.shape[1]
    channel = first_channel + lax.broadcasted_iota(jnp.int32, (1, width), 1)
    group_index = channel // (pool_total // group_count)
    window_len = jnp.left_shift(jnp.int32(2), group_index)
    running = jnp.zeros((row_count, width), jnp.float32)
    for offset in range(halo_rows):
        shifted = extended[halo_rows - offset:halo_rows - offset + row_count]
        running = running + jnp.where(offset < window_len, shifted, 0.0)
    position = first_pos + lax.broadcasted_iota(jnp.int32, (row_count, 1), 0)
    divisor = jnp.minimum(position + 1, window_len).astype(jnp.float32)
    return running / divisor - extended[halo_rows:]

def reference(inputs, norm_gain, in_weight, pool_scale, out_weight):
    current = inputs
    for layer_index in range(LAYERS):
        widened = current.astype(jnp.float32)
        inv_rms = lax.rsqrt(lax.optimization_barrier(jnp.mean(widened * widened, axis=1, keepdims=True)) + epsilon)
        normed = (widened * inv_rms * norm_gain[layer_index]).astype(jnp.bfloat16)
        pool_in = jnp.dot(normed, in_weight[layer_index], preferred_element_type=jnp.float32).astype(jnp.bfloat16)
        extended = jnp.concatenate([jnp.zeros((halo_rows, P_SIZE), jnp.float32), pool_in.astype(jnp.float32)], 0)
        means = window_means(extended, TOKENS, 0, 0, P_SIZE)
        mixed = (means * pool_scale[layer_index]).astype(jnp.bfloat16)
        branch = jnp.dot(mixed, out_weight[layer_index], preferred_element_type=jnp.float32)
        current = (widened + branch).astype(jnp.bfloat16)
    return current
```

```python
import functools

import jax
import jax.numpy as jnp
from jax import lax
from jax.experimental import pallas as pl
from jax.experimental.pallas import tpu as pltpu
from jax.sharding import PartitionSpec as P

D = 4096
P_SIZE = 1024
LAYERS = 3
EPS = 1e-06
HALO = 16
NZ, NY, NT = 16, 4, 8
MESH = pl.DeviceIdType.MESH
BF16, F32 = jnp.bfloat16, jnp.float32


def remote(src, dst, send, recv, sp, tp):
    return pltpu.make_async_remote_copy(
        src_ref=src, dst_ref=dst, send_sem=send, recv_sem=recv,
        device_id=(sp, tp), device_id_type=MESH,
    )


def kernel(
    x_ref, gain_ref, win_ref, scale_ref, wout_ref, out_ref,
    wi, wo, state, part, rs_in, ssq, mixed, mix_in, tail, halo,
    z_send, z_recv, y_send, y_recv, rs_send, rs_recv,
    sq_send, sq_recv, mx_send, mx_recv, h_send, h_recv, own_sem,
):
    sp = lax.axis_index("sp")
    t = lax.axis_index("tp")
    z, y = sp // NY, sp % NY

    def at(zz, yy):
        return ((zz + NZ) % NZ) * NY + (yy + NY) % NY

    z_up, z_down = at(z + 1, y), at(z - 1, y)
    y_up, y_down = at(z, y + 1), at(z, y - 1)
    sp_next, sp_prev = (sp + 1) % (NZ * NY), (sp + NZ * NY - 1) % (NZ * NY)

    barrier = pltpu.get_barrier_semaphore()
    for peer in (z_up, z_down, y_up, y_down, sp_next, sp_prev):
        pl.semaphore_signal(barrier, inc=1, device_id=(peer, t), device_id_type=MESH)
    for d in range(1, NT):
        pl.semaphore_signal(
            barrier, inc=1, device_id=(sp, (t + d) % NT), device_id_type=MESH
        )

    own = []
    for layer in range(LAYERS):
        own.append(pltpu.make_async_copy(win_ref.at[layer], wi.at[layer, z, y], own_sem.at[2 * layer]))
        own.append(pltpu.make_async_copy(wout_ref.at[layer], wo.at[layer, z, y], own_sem.at[2 * layer + 1]))
    for copy in own:
        copy.start()
    for copy in own:
        copy.wait()
    pl.semaphore_wait(barrier, 6 + NT - 1)

    sent = []

    def go(copy):
        copy.start()
        sent.append(copy)
        return copy

    def piece_of(p):
        layer, kind = p // 2, p % 2
        return (wo if kind else wi).at[layer]

    def z_copy(p, direction, step, whole):
        buf = piece_of(p)
        block = (z - step + NZ) % NZ if direction == 0 else (z + step) % NZ
        ref = buf.at[block] if whole else buf.at[block, y]
        return remote(
            ref, ref, z_send.at[p, direction, step], z_recv.at[p, direction, step],
            z_up if direction == 0 else z_down, t,
        )

    def z_wait(p, direction, step, whole):
        z_copy(p, direction, step, whole).wait_recv()

    def y_copy(p, slot, whole):
        buf = piece_of(p)
        up = (y + 1) % NY
        down = (y + NY - 1) % NY
        if whole:
            refs = (buf.at[:, y], buf.at[:, y], buf.at[pl.ds(0, 8), down], buf.at[pl.ds(8, 8), up])
        else:
            half = 256
            refs = (
                buf.at[z, y], buf.at[z, y],
                buf.at[z, down, :, pl.ds(0, half)], buf.at[z, up, :, pl.ds(half, half)],
            )
        ref = refs[slot]
        return remote(
            ref, ref, y_send.at[p, slot], y_recv.at[p, slot], y_up if slot % 2 == 0 else y_down, t
        )

    def stage(p, k):
        z_first = p % 3 != 2
        if z_first:
            if 1 <= k <= 8:
                z_wait(p, 0, k - 1, False)
            if 1 <= k <= 7:
                z_wait(p, 1, k - 1, False)
            if k <= 7:
                go(z_copy(p, 0, k, False))
            if k <= 6:
                go(z_copy(p, 1, k, False))
            y0, whole = 8, True
        else:
            s = k - 2
            y0, whole = 0, False
        if k == y0:
            go(y_copy(p, 0, whole))
            go(y_copy(p, 1, whole))
        if k == y0 + 1:
            y_copy(p, 0, whole).wait_recv()
            y_copy(p, 1, whole).wait_recv()
            go(y_copy(p, 2, whole))
            go(y_copy(p, 3, whole))
        if k == y0 + 2:
            y_copy(p, 2, whole).wait_recv()
            y_copy(p, 3, whole).wait_recv()
        if not z_first:
            if 1 <= s <= 8:
                z_wait(p, 0, s - 1, True)
            if 1 <= s <= 7:
                z_wait(p, 1, s - 1, True)
            if 0 <= s <= 7:
                go(z_copy(p, 0, s, True))
            if 0 <= s <= 6:
                go(z_copy(p, 1, s, True))

    for k in range(11):
        for p in range(2 * LAYERS):
            stage(p, k)

    lane0 = t * (D // NT)
    state[...] = x_ref[...]
    row = lax.broadcasted_iota(jnp.int32, (256, 128), 0)
    group = t // 2
    window = jnp.left_shift(jnp.int32(2), group)
    position = sp * 256 + row
    inverse = 1.0 / jnp.minimum(position + 1, window).astype(F32)

    for layer in range(LAYERS):
        wide = state[...].astype(F32)
        squares = jnp.sum(wide * wide, axis=1, keepdims=True)
        squares = jnp.broadcast_to(squares, (256, 128)).T[0:1, :]
        ssq[layer, t] = squares
        for d in range(1, NT):
            go(remote(
                ssq.at[layer, t], ssq.at[layer, t],
                sq_send.at[layer, d], sq_recv.at[layer, d], sp, (t + d) % NT,
            ))
        own_gain = gain_ref[pl.ds(layer, 1), pl.ds(pl.multiple_of(lane0, 128), D // NT)]
        scaled = (wide * own_gain).astype(BF16)
        weights = wi[layer].reshape(P_SIZE, D // NT)
        partial = lax.dot_general(
            scaled, weights, (((1,), (1,)), ((), ())), preferred_element_type=F32
        ).astype(BF16)
        for j in range(NT):
            part[layer, j] = partial[:, j * 128:(j + 1) * 128]
        for d in range(1, NT):
            j = (t + d) % NT
            go(remote(
                part.at[layer, j], rs_in.at[layer, d],
                rs_send.at[layer, d], rs_recv.at[layer, d], sp, j,
            ))
        total = part[layer, t].astype(F32)
        for d in range(1, NT):
            remote(
                ssq.at[layer, t], ssq.at[layer, t],
                sq_send.at[layer, d], sq_recv.at[layer, d], sp, t,
            ).wait_recv()
        all_squares = jnp.sum(ssq[layer], axis=0)
        inv_rms = lax.rsqrt(all_squares / D + EPS)
        inv_rms = jnp.broadcast_to(inv_rms, (128, 256)).T
        for d in range(1, NT):
            remote(
                part.at[layer, 0], rs_in.at[layer, d],
                rs_send.at[layer, d], rs_recv.at[layer, d], sp, t,
            ).wait_recv()
            total = total + rs_in[layer, d].astype(F32)
        pool_in = (total * inv_rms).astype(BF16)
        tail[layer] = pool_in[256 - HALO:]
        edge = go(remote(
            tail.at[layer], halo.at[layer], h_send.at[layer], h_recv.at[layer], sp_next, t
        ))
        pool_in = pool_in.astype(F32)
        edge.wait_recv()
        before = halo[layer].astype(F32) * (sp > 0).astype(F32)
        run = jnp.concatenate([before, pool_in], axis=0)
        picked = None
        for g in range(4):
            run = run + pltpu.roll(run, 1 << g, 0)
            picked = run if g == 0 else jnp.where(group >= g, run, picked)
        means = picked[HALO:] * inverse - pool_in
        own_scale = scale_ref[pl.ds(layer, 1), pl.ds(pl.multiple_of(t * 128, 128), 128)]
        mixed[layer] = (means * own_scale).astype(BF16)
        for d in range(1, NT):
            go(remote(
                mixed.at[layer], mix_in.at[layer, t],
                mx_send.at[layer, d], mx_recv.at[layer, d], sp, (t + d) % NT,
            ))
        mix_in[layer, t] = mixed[layer]
        for d in range(1, NT):
            remote(
                mixed.at[layer], mix_in.at[layer, t],
                mx_send.at[layer, d], mx_recv.at[layer, d], sp, t,
            ).wait_recv()
        pooled = jnp.concatenate([mix_in[layer, k] for k in range(NT)], axis=1)
        branch = jnp.dot(
            pooled, wo[layer].reshape(P_SIZE, D // NT), preferred_element_type=F32
        )
        state[...] = (wide + branch).astype(BF16)

    out_ref[...] = state[...]
    for copy in sent:
        copy.wait_send()


def body(inputs, norm_gain, in_weight, pool_scale, out_weight):
    rows, features = inputs.shape
    vmem = pl.BlockSpec(memory_space=pltpu.VMEM)
    dma = pltpu.SemaphoreType.DMA
    pieces = 2 * LAYERS
    gathered = pltpu.VMEM((LAYERS, NZ, NY, P_SIZE // 64, features), BF16)
    blocks = pltpu.VMEM((LAYERS, NT, rows, 128), BF16)
    return pl.pallas_call(
        kernel,
        out_shape=jax.ShapeDtypeStruct(inputs.shape, inputs.dtype),
        in_specs=[vmem] * 5,
        out_specs=vmem,
        scratch_shapes=[
            gathered, gathered,
            pltpu.VMEM((rows, features), BF16),
            blocks, blocks,
            pltpu.VMEM((LAYERS, NT, 1, rows), F32),
            pltpu.VMEM((LAYERS, rows, 128), BF16),
            blocks,
            pltpu.VMEM((LAYERS, HALO, 128), BF16),
            pltpu.VMEM((LAYERS, HALO, 128), BF16),
            dma((pieces, 2, 8)), dma((pieces, 2, 8)),
            dma((pieces, 4)), dma((pieces, 4)),
            dma((LAYERS, NT)), dma((LAYERS, NT)),
            dma((LAYERS, NT)), dma((LAYERS, NT)),
            dma((LAYERS, NT)), dma((LAYERS, NT)),
            dma((LAYERS,)), dma((LAYERS,)),
            dma((pieces,)),
        ],
        compiler_params=pltpu.CompilerParams(
            collective_id=0, has_side_effects=True, vmem_limit_bytes=40 * 1024 * 1024
        ),
        name="mixer",
    )(inputs, norm_gain, jnp.swapaxes(in_weight, 1, 2), pool_scale, out_weight)


def solution(mesh):
    placed = (P("sp", "tp"), P(), P(None, "tp", "sp"), P(), P(None, "sp", "tp"))
    return jax.shard_map(body, mesh=mesh, in_specs=placed, out_specs=P("sp", "tp"), check_vma=False)
```

```python
import functools

import jax
import jax.numpy as jnp
from jax import lax
from jax.experimental import pallas as pl
from jax.experimental.pallas import tpu as pltpu
from jax.sharding import PartitionSpec as P

D = 4096
P_SIZE = 1024
LAYERS = 3
EPS = 1e-06
HALO = 16
NZ, NY, NT = 16, 4, 8
MESH = pl.DeviceIdType.MESH
BF16, F32 = jnp.bfloat16, jnp.float32


VMEM_LIMIT = 60 * 1024 * 1024
OTHERS = (4, 5, 2, 3, 6, 7, 1)
RELAYS = ((-6, (2, 1, -1)), (6, (1, -1)), (-2, (2, 1, -1)), (2, (-2, -1, 1)))
FIRST = (2, -6, -2, 6)
LATER = (1, -1, 3, -3, 4, -4, 5, -5, 7, -7, 8)
PLAN = {
    "start": ((0, 0), (0, 1), (1, 0), (0, 2), (1, 1), (2, 0), (0, 3), (1, 2), (2, 1), (0, 4)),
    ("b", 0): ((1, 3), (2, 2), (3, 0)),
    ("c", 0): ((2, 3), (3, 1), (4, 0)),
    ("d", 0): ((1, 4),),
    ("a", 1): ((2, 4),),
    ("b", 1): ((3, 2), (4, 1), (5, 0), (3, 3), (4, 2), (5, 1)),
    ("c", 1): ((4, 3), (5, 2)),
    ("d", 1): ((3, 4),),
    ("a", 2): ((4, 4),),
    ("b", 2): ((5, 3),),
    ("d", 2): ((5, 4),),
}


def remote(src, dst, send, recv, sp, tp):
    return pltpu.make_async_remote_copy(
        src_ref=src, dst_ref=dst, send_sem=send, recv_sem=recv,
        device_id=(sp, tp), device_id_type=MESH,
    )


def kernel(
    x_ref, gain_ref, win_ref, scale_ref, wout_ref, out_ref,
    wi, wo, state, gain, scale, part, rs_in, ssq, mixed, mix_in, tail, halo,
    z_send, z_recv, y_send, y_recv, rs_send, rs_recv,
    sq_send, sq_recv, mx_send, mx_recv, h_send, h_recv, own_sem,
):
    sp = lax.axis_index("sp")
    t = lax.axis_index("tp")
    z, y = sp // NY, sp % NY

    def at(zz, yy):
        return ((zz + NZ) % NZ) * NY + (yy + NY) % NY

    def peer(d):
        return ((t // 2 + d // 2) % 4) * 2 + (t + d) % 2

    sp_next, sp_prev = (sp + 1) % (NZ * NY), (sp + NZ * NY - 1) % (NZ * NY)

    barrier = pltpu.get_barrier_semaphore()
    greeted = [at(z + o, y) for o in (1, -1, 2, -2, 6, -6)]
    greeted += [at(z, y + 1), at(z, y - 1), sp_next, sp_prev]
    for to in greeted:
        pl.semaphore_signal(barrier, inc=1, device_id=(to, t), device_id_type=MESH)
    for d in OTHERS:
        pl.semaphore_signal(barrier, inc=1, device_id=(sp, peer(d)), device_id_type=MESH)

    own = []
    for layer in range(LAYERS):
        own.append(pltpu.make_async_copy(win_ref.at[layer], wi.at[layer, z, y], own_sem.at[2 * layer]))
        own.append(pltpu.make_async_copy(wout_ref.at[layer], wo.at[layer, z, y], own_sem.at[2 * layer + 1]))
    own.append(pltpu.make_async_copy(x_ref, state, own_sem.at[6]))
    own.append(pltpu.make_async_copy(gain_ref, gain, own_sem.at[7]))
    own.append(pltpu.make_async_copy(scale_ref, scale, own_sem.at[8]))
    for copy in own:
        copy.start()
    for copy in own:
        copy.wait()
    pl.semaphore_wait(barrier, len(greeted) + NT - 1)

    sent = []

    def go(copy):
        copy.start()
        sent.append(copy)
        return copy

    def piece(p):
        return (wo if p % 2 else wi).at[p // 2]

    def line(offset):
        return (z + offset + 2 * NZ) % NZ

    def along_z(p, offset, way, slot):
        block = piece(p).at[line(offset), y]
        go(remote(block, block, z_send.at[p, slot], z_recv.at[p, slot], at(z + way, y), t))

    def along_y(p, offset, from_y, way, slot):
        block = piece(p).at[line(offset), (y + from_y + NY) % NY]
        go(remote(block, block, y_send.at[p, slot], y_recv.at[p, slot], at(z, y + way), t))

    def arrived(p, sems, slot, count):
        blocks = piece(p).at[pl.ds(0, count), 0]
        remote(blocks, blocks, sems[0].at[p, slot], sems[1].at[p, slot], sp, t).wait_recv()

    zs, ys = (z_send, z_recv), (y_send, y_recv)

    def stage(p, k):
        if k == 0:
            for way in (6, -6, 2, -2):
                along_z(p, 0, way, 0)
            for way in (1, -1):
                along_y(p, 0, 0, way, 0 if way > 0 else 1)
        if k == 1:
            arrived(p, zs, 0, 4)
            for offset, ways in RELAYS:
                for way in ways:
                    along_z(p, offset, way, 1)
            for way in (1, -1):
                for offset in FIRST:
                    along_y(p, offset, 0, way, 2 if way > 0 else 3)
        if k == 2:
            arrived(p, zs, 1, 11)
            for way in (1, -1):
                for offset in LATER:
                    along_y(p, offset, 0, way, 4 if way > 0 else 5)
            for slot in (0, 1):
                arrived(p, ys, slot, 1)
                arrived(p, ys, slot + 2, 4)
            for offset in (0, 2, -6):
                along_y(p, offset, -1, 1, 6)
            for offset in (-2, 6):
                along_y(p, offset, 1, -1, 7)
        if k == 3:
            arrived(p, ys, 4, 11)
            arrived(p, ys, 5, 11)
            for offset in LATER[:5]:
                along_y(p, offset, -1, 1, 8)
            for offset in LATER[5:]:
                along_y(p, offset, 1, -1, 9)
        if k == 4:
            for slot, count in ((6, 3), (7, 2), (8, 5), (9, 6)):
                arrived(p, ys, slot, count)

    def advance(stages):
        for p, k in stages:
            stage(p, k)

    advance(PLAN["start"])

    lane0 = t * (D // NT)
    row = lax.broadcasted_iota(jnp.int32, (256, 128), 0)
    group = t // 2
    window = jnp.left_shift(jnp.int32(2), group)
    position = sp * 256 + row
    inverse = 1.0 / jnp.minimum(position + 1, window).astype(F32)

    for layer in range(LAYERS):
        wide = state[...].astype(F32)
        squares = jnp.sum(wide * wide, axis=1, keepdims=True)
        squares = jnp.broadcast_to(squares, (256, 128)).T[0:1, :]
        ssq[layer, t] = squares
        for d in OTHERS:
            go(remote(
                ssq.at[layer, t], ssq.at[layer, t],
                sq_send.at[layer, d], sq_recv.at[layer, d], sp, peer(d),
            ))
        advance(PLAN.get(("a", layer), ()))
        own_gain = gain[pl.ds(layer, 1), pl.ds(pl.multiple_of(lane0, 128), D // NT)]
        scaled = (wide * own_gain).astype(BF16)
        weights = wi[layer].reshape(P_SIZE, D // NT)
        partial = lax.dot_general(
            scaled, weights, (((1,), (1,)), ((), ())), preferred_element_type=F32
        ).astype(BF16)
        for j in range(NT):
            part[layer, j] = partial[:, j * 128:(j + 1) * 128]
        for d in OTHERS:
            j = peer(d)
            go(remote(
                part.at[layer, j], rs_in.at[layer, d],
                rs_send.at[layer, d], rs_recv.at[layer, d], sp, j,
            ))
        advance(PLAN.get(("b", layer), ()))
        total = part[layer, t].astype(F32)
        for d in OTHERS:
            remote(
                ssq.at[layer, t], ssq.at[layer, t],
                sq_send.at[layer, d], sq_recv.at[layer, d], sp, t,
            ).wait_recv()
        all_squares = jnp.sum(ssq[layer], axis=0)
        inv_rms = lax.rsqrt(all_squares / D + EPS)
        inv_rms = jnp.broadcast_to(inv_rms, (128, 256)).T
        for d in OTHERS:
            remote(
                part.at[layer, 0], rs_in.at[layer, d],
                rs_send.at[layer, d], rs_recv.at[layer, d], sp, t,
            ).wait_recv()
            total = total + rs_in[layer, d].astype(F32)
        pool_in = (total * inv_rms).astype(BF16)
        tail[layer] = pool_in[256 - HALO:]
        edge = go(remote(
            tail.at[layer], halo.at[layer], h_send.at[layer], h_recv.at[layer], sp_next, t
        ))
        pool_in = pool_in.astype(F32)
        edge.wait_recv()
        before = halo[layer].astype(F32) * (sp > 0).astype(F32)
        run = jnp.concatenate([before, pool_in], axis=0)
        picked = None
        for g in range(4):
            run = run + pltpu.roll(run, 1 << g, 0)
            picked = run if g == 0 else jnp.where(group >= g, run, picked)
        means = picked[HALO:] * inverse - pool_in
        own_scale = scale[pl.ds(layer, 1), pl.ds(pl.multiple_of(t * 128, 128), 128)]
        mixed[layer] = (means * own_scale).astype(BF16)
        for d in OTHERS:
            go(remote(
                mixed.at[layer], mix_in.at[layer, t],
                mx_send.at[layer, d], mx_recv.at[layer, d], sp, peer(d),
            ))
        mix_in[layer, t] = mixed[layer]
        advance(PLAN.get(("c", layer), ()))
        for d in OTHERS:
            remote(
                mixed.at[layer], mix_in.at[layer, t],
                mx_send.at[layer, d], mx_recv.at[layer, d], sp, t,
            ).wait_recv()
        advance(PLAN.get(("d", layer), ()))
        pooled = jnp.concatenate([mix_in[layer, k] for k in range(NT)], axis=1)
        branch = jnp.dot(
            pooled, wo[layer].reshape(P_SIZE, D // NT), preferred_element_type=F32
        )
        state[...] = (wide + branch).astype(BF16)

    out_ref[...] = state[...]
    for copy in sent:
        copy.wait_send()


def body(inputs, norm_gain, in_weight, pool_scale, out_weight):
    rows, features = inputs.shape
    vmem = pl.BlockSpec(memory_space=pltpu.VMEM)
    hbm = pl.BlockSpec(memory_space=pl.ANY)
    dma = pltpu.SemaphoreType.DMA
    pieces = 2 * LAYERS
    gathered = pltpu.VMEM((LAYERS, NZ, NY, P_SIZE // 64, features), BF16)
    blocks = pltpu.VMEM((LAYERS, NT, rows, 128), BF16)
    return pl.pallas_call(
        kernel,
        out_shape=jax.ShapeDtypeStruct(inputs.shape, inputs.dtype),
        in_specs=[hbm] * 5,
        out_specs=vmem,
        scratch_shapes=[
            gathered, gathered,
            pltpu.VMEM((rows, features), BF16),
            pltpu.VMEM(norm_gain.shape, F32),
            pltpu.VMEM(pool_scale.shape, F32),
            blocks, blocks,
            pltpu.VMEM((LAYERS, NT, 1, rows), F32),
            pltpu.VMEM((LAYERS, rows, 128), BF16),
            blocks,
            pltpu.VMEM((LAYERS, HALO, 128), BF16),
            pltpu.VMEM((LAYERS, HALO, 128), BF16),
            dma((pieces, 2)), dma((pieces, 2)),
            dma((pieces, 10)), dma((pieces, 10)),
            dma((LAYERS, NT)), dma((LAYERS, NT)),
            dma((LAYERS, NT)), dma((LAYERS, NT)),
            dma((LAYERS, NT)), dma((LAYERS, NT)),
            dma((LAYERS,)), dma((LAYERS,)),
            dma((pieces + 3,)),
        ],
        compiler_params=pltpu.CompilerParams(
            collective_id=0, has_side_effects=True, vmem_limit_bytes=VMEM_LIMIT
        ),
        name="mixer",
    )(inputs, norm_gain, jnp.swapaxes(in_weight, 1, 2), pool_scale, out_weight)


def solution(mesh):
    placed = (P("sp", "tp"), P(), P(None, "tp", "sp"), P(), P(None, "sp", "tp"))
    return jax.shard_map(body, mesh=mesh, in_specs=placed, out_specs=P("sp", "tp"), check_vma=False)
```

```python
import functools

import jax
import jax.numpy as jnp
from jax import lax
from jax.experimental import pallas as pl
from jax.experimental.pallas import tpu as pltpu
from jax.sharding import PartitionSpec as P

D = 4096
P_SIZE = 1024
LAYERS = 3
EPS = 1e-06
HALO = 16
AHEAD, SPLIT = 48, 112
NZ, NY, NT = 16, 4, 8
MESH = pl.DeviceIdType.MESH
BF16, F32 = jnp.bfloat16, jnp.float32


VMEM_LIMIT = 60 * 1024 * 1024
OTHERS = (4, 5, 2, 3, 6, 7, 1)
RELAYS = ((-6, (2, 1, -1)), (6, (1, -1)), (-2, (2, 1, -1)), (2, (-2, -1, 1)))
FIRST = (2, -6, -2, 6)
LATER = (1, -1, 3, -3, 4, -4, 5, -5, 7, -7, 8)
ROUND = (4, 5)
PLAN = {
    "start": (
        (0, 0), (4, 0), (5, 0), (1, 0), (0, 1), (4, 1), (5, 1), (2, 0), (1, 1),
        (0, 2), (4, 2), (3, 0), (0, 3), (2, 1), (1, 2), (5, 2), (4, 3), (0, 4),
    ),
    ("mid", 0): ((5, 3),),
    ("pool0", 0): ((3, 1), (4, 4), (1, 3), (2, 2)),
    ("pool1", 0): ((4, 5), (5, 4)),
    ("out0", 0): ((1, 4), (4, 6), (5, 5), (2, 3), (3, 2)),
    ("in0", 1): ((2, 4),),
    ("out1", 0): ((4, 7), (5, 6)),
    ("pool0", 1): ((3, 3), (4, 8), (5, 7)),
    ("pool1", 1): ((4, 9), (5, 8)),
    ("out0", 1): ((3, 4), (4, 10), (5, 9)),
    ("out1", 1): ((5, 10),),
}


def remote(src, dst, send, recv, sp, tp):
    return pltpu.make_async_remote_copy(
        src_ref=src, dst_ref=dst, send_sem=send, recv_sem=recv,
        device_id=(sp, tp), device_id_type=MESH,
    )


def kernel(
    x_ref, gain_ref, win_ref, scale_ref, wout_ref, out_ref,
    wi, wo, state, gain, scale, inverse, part, rs_in, ssq, mixed, mix_in,
    z_send, z_recv, y_send, y_recv, rs_send, rs_recv,
    sq_send, sq_recv, mx_send, mx_recv, h_send, h_recv, own_sem, r_recv,
):
    sp = lax.axis_index("sp")
    t = lax.axis_index("tp")
    z, y = sp // NY, sp % NY

    def at(zz, yy):
        return ((zz + NZ) % NZ) * NY + (yy + NY) % NY

    def peer(d):
        return ((t // 2 + d // 2) % 4) * 2 + (t + d) % 2

    sp_next, sp_prev = (sp + 1) % (NZ * NY), (sp + NZ * NY - 1) % (NZ * NY)

    barrier = pltpu.get_barrier_semaphore()
    greeted = [at(z + o, y) for o in (1, -1, 2, -2, 6, -6)]
    greeted += [at(z, y + 1), at(z, y - 1), sp_next, sp_prev]
    for to in greeted:
        pl.semaphore_signal(barrier, inc=1, device_id=(to, t), device_id_type=MESH)
    for d in OTHERS:
        pl.semaphore_signal(barrier, inc=1, device_id=(sp, peer(d)), device_id_type=MESH)

    own = []
    for layer in range(LAYERS):
        own.append(pltpu.make_async_copy(win_ref.at[layer], wi.at[layer, z, y], own_sem.at[0]))
        own.append(pltpu.make_async_copy(wout_ref.at[layer], wo.at[layer, z, y], own_sem.at[0]))
    own.append(pltpu.make_async_copy(x_ref, state.at[pl.ds(AHEAD, 256)], own_sem.at[1]))
    own.append(pltpu.make_async_copy(gain_ref, gain, own_sem.at[2]))
    own.append(pltpu.make_async_copy(scale_ref, scale, own_sem.at[3]))
    for copy in own:
        copy.start()
    six = wi.at[0, pl.ds(0, 2 * LAYERS), 0]
    pltpu.make_async_copy(six, six, own_sem.at[0]).wait()
    for copy in own[2 * LAYERS:]:
        copy.wait()
    pl.semaphore_wait(barrier, len(greeted) + NT - 1)

    def piece(p):
        return (wo if p % 2 else wi).at[p // 2]

    def line(offset):
        return (z + offset + 2 * NZ) % NZ

    def along_z(p, offset, way, slot):
        block = piece(p).at[line(offset), y]
        remote(block, block, z_send.at[p], z_recv.at[p, slot], at(z + way, y), t).start()

    def along_y(p, offset, from_y, way, slot):
        block = piece(p).at[line(offset), (y + from_y + NY) % NY]
        remote(block, block, y_send.at[p], y_recv.at[p, slot], at(z, y + way), t).start()

    def landed(blocks, sem):
        remote(blocks, blocks, sem, sem, sp, t).wait_recv()

    def stage(p, k):
        if k == 0:
            for way in (6, -6, 2, -2):
                along_z(p, 0, way, 0)
            for way in (1, -1):
                along_y(p, 0, 0, way, 0)
        if k == 1:
            landed(piece(p).at[pl.ds(0, 4), 0], z_recv.at[p, 0])
            for offset, ways in RELAYS:
                for way in ways:
                    along_z(p, offset, way, 1)
            for way in (1, -1):
                for offset in FIRST:
                    along_y(p, offset, 0, way, 0)
        if k == 2:
            landed(piece(p).at[pl.ds(0, 11), 0], z_recv.at[p, 1])
            for way in (1, -1):
                for offset in LATER:
                    along_y(p, offset, 0, way, 1)
            landed(piece(p).at[pl.ds(0, 5), pl.ds(0, 2)], y_recv.at[p, 0])
            for offset in (0, 2, -6):
                along_y(p, offset, -1, 1, 2)
            for offset in (-2, 6):
                along_y(p, offset, 1, -1, 2)
        if k == 3:
            landed(piece(p).at[pl.ds(0, 11), pl.ds(0, 2)], y_recv.at[p, 1])
            for offset in LATER[:5]:
                along_y(p, offset, -1, 1, 2)
            for offset in LATER[5:]:
                along_y(p, offset, 1, -1, 2)
        if k == 4:
            landed(piece(p).at[:, 0], y_recv.at[p, 2])

    def ring_copy(p, way, step):
        row = piece(p).at[line(-way * step)]
        remote(
            row, row, z_send.at[p], r_recv.at[p - ROUND[0], step], at(z + way, y), t
        ).start()

    def ring_stage(p, k):
        if k == 0:
            for way in (1, -1):
                along_y(p, 0, 0, way, 0)
        if k == 1:
            landed(piece(p).at[pl.ds(0, 2), 0], y_recv.at[p, 0])
            for way in (1, -1):
                half = piece(p).at[z, (y - way + NY) % NY, :, pl.ds(128 + 128 * way, 256)]
                remote(half, half, y_send.at[p], y_recv.at[p, 1], at(z, y + way), t).start()
        if k == 2:
            landed(piece(p).at[0, 0], y_recv.at[p, 1])
        if 3 <= k <= 10:
            landed(piece(p).at[pl.ds(0, 2 if k < 10 else 1)], r_recv.at[p - ROUND[0], k - 3])
        for way, steps in ((1, 8), (-1, 7)):
            if 2 <= k < 2 + steps:
                ring_copy(p, way, k - 2)

    def advance(*where):
        for p, k in PLAN.get(where[0] if len(where) == 1 else where, ()):
            if p in ROUND:
                ring_stage(p, k)
            else:
                stage(p, k)

    ahead = remote(
        x_ref.at[pl.ds(256 - AHEAD, AHEAD)], state.at[pl.ds(0, AHEAD)],
        h_send.at[0], h_recv.at[0], sp_next, t,
    )
    ahead.start()
    window = jnp.left_shift(jnp.int32(2), t // 2)
    position = sp * 256 - AHEAD + lax.broadcasted_iota(jnp.int32, inverse.shape, 0)
    count = jnp.maximum(jnp.minimum(position + 1, window), 1)
    inverse[...] = 1.0 / count.astype(F32)
    advance("start")
    ahead.wait_recv()
    first = state[0:AHEAD].astype(F32) * (sp > 0).astype(F32)
    state[0:AHEAD] = first.astype(BF16)

    lane0 = pl.multiple_of(t * (D // NT), 128)
    lane1 = pl.multiple_of(t * 128, 128)
    group = t // 2

    def rows_in(h, layer):
        return (HALO * layer, AHEAD + SPLIT - HALO * layer) if h == 0 else (AHEAD + SPLIT, 256 - SPLIT)

    def rows_out(h, layer):
        start, count = rows_in(h, layer)
        return (start, count) if h else (start + HALO, count - HALO)

    def part_copy(h, layer, d, j):
        rows = pl.ds(0, rows_in(h, layer)[1])
        return remote(
            part.at[layer, h, j, rows], rs_in.at[layer, h, d, rows],
            rs_send.at[layer, h], rs_recv.at[layer, h], sp, j,
        )

    def square_copy(h, layer, d, j):
        return remote(
            ssq.at[layer, h, t], ssq.at[layer, h, t],
            sq_send.at[layer, h], sq_recv.at[layer, h], sp, j,
        )

    def mixed_copy(h, layer, d, j):
        rows = pl.ds(0, rows_out(h, layer)[1])
        return remote(
            mixed.at[layer, h, rows], mix_in.at[layer, h, t, rows],
            mx_send.at[layer, h], mx_recv.at[layer, h], sp, j,
        )

    def project_in(h, layer):
        start, count = rows_in(h, layer)
        wide = state[start:start + count].astype(F32)
        squares = jnp.sum(wide * wide, axis=1, keepdims=True)
        squares = jnp.broadcast_to(squares, (count, 128))
        squares = jnp.concatenate([squares, jnp.zeros((256 - count, 128), F32)], axis=0)
        ssq[layer, h, t] = squares.T[0:1, :]
        for d in OTHERS:
            square_copy(h, layer, d, peer(d)).start()
        own_gain = gain[pl.ds(layer, 1), pl.ds(lane0, D // NT)]
        scaled = (wide * own_gain).astype(BF16)
        weights = wi[layer].reshape(P_SIZE, D // NT)
        partial = lax.dot_general(
            scaled, weights, (((1,), (1,)), ((), ())), preferred_element_type=F32
        ).astype(BF16)
        for j in range(NT):
            part[layer, h, j, 0:count] = partial[:, j * 128:(j + 1) * 128]
        for d in OTHERS:
            part_copy(h, layer, d, peer(d)).start()

    def pool(h, layer, tail):
        count = rows_in(h, layer)[1]
        start, out_count = rows_out(h, layer)
        seven = pl.ds(0, NT - 1)
        landed(ssq.at[layer, h, seven], sq_recv.at[layer, h])
        inv_rms = lax.rsqrt(jnp.sum(ssq[layer, h], axis=0) / D + EPS)
        inv_rms = jnp.broadcast_to(inv_rms, (128, 256)).T[0:count]
        total = part[layer, h, t, 0:count].astype(F32)
        landed(rs_in.at[layer, h, seven, pl.ds(0, count)], rs_recv.at[layer, h])
        for d in OTHERS:
            total = total + rs_in[layer, h, d, 0:count].astype(F32)
        pool_in = (total * inv_rms).astype(BF16).astype(F32)
        run = pool_in if tail is None else jnp.concatenate([tail, pool_in], axis=0)
        own = run[HALO:]
        picked = None
        for g in range(4):
            run = run + pltpu.roll(run, 1 << g, 0)
            picked = run if g == 0 else jnp.where(group >= g, run, picked)
        means = picked[HALO:] * inverse[start:start + out_count] - own
        own_scale = scale[pl.ds(layer, 1), pl.ds(lane1, 128)]
        mixed[layer, h, 0:out_count] = (means * own_scale).astype(BF16)
        for d in OTHERS:
            mixed_copy(h, layer, d, peer(d)).start()
        mix_in[layer, h, t, 0:out_count] = mixed[layer, h, 0:out_count]
        return pool_in[count - HALO:]

    def project_out(h, layer):
        start, count = rows_out(h, layer)
        landed(mix_in.at[layer, h, pl.ds(0, NT - 1), pl.ds(0, count)], mx_recv.at[layer, h])
        pooled = jnp.concatenate(
            [mix_in[layer, h, k, 0:count] for k in range(NT)], axis=1
        )
        branch = jnp.dot(
            pooled, wo[layer].reshape(P_SIZE, D // NT), preferred_element_type=F32
        )
        after = (state[start:start + count].astype(F32) + branch).astype(BF16)
        if layer == LAYERS - 1:
            out_ref[start - AHEAD:start - AHEAD + count] = after
        else:
            state[start:start + count] = after

    project_in(0, 0)
    advance("mid", 0)
    project_in(1, 0)
    for layer in range(LAYERS):
        advance("pool0", layer)
        tail = pool(0, layer, None)
        advance("pool1", layer)
        pool(1, layer, tail)
        advance("out0", layer)
        project_out(0, layer)
        if layer < LAYERS - 1:
            advance("in0", layer + 1)
            project_in(0, layer + 1)
        advance("out1", layer)
        project_out(1, layer)
        if layer < LAYERS - 1:
            project_in(1, layer + 1)

    def left(blocks, sem):
        remote(blocks, blocks, sem, sem, sp, t).wait_send()

    ahead.wait_send()
    for p in range(2 * LAYERS):
        if p in ROUND:
            left(piece(p).at[pl.ds(0, 15)], z_send.at[p])
            left(piece(p).at[pl.ds(0, 3), 0], y_send.at[p])
        else:
            left(piece(p).at[pl.ds(0, 15), 0], z_send.at[p])
            left(piece(p).at[pl.ds(0, 12)], y_send.at[p])
    seven = pl.ds(0, NT - 1)
    for layer in range(LAYERS):
        for h in (0, 1):
            count, out_count = rows_in(h, layer)[1], rows_out(h, layer)[1]
            left(ssq.at[layer, h, seven], sq_send.at[layer, h])
            left(part.at[layer, h, seven, pl.ds(0, count)], rs_send.at[layer, h])
            left(mix_in.at[layer, h, seven, pl.ds(0, out_count)], mx_send.at[layer, h])


def body(inputs, norm_gain, in_weight, pool_scale, out_weight):
    rows, features = inputs.shape
    vmem = pl.BlockSpec(memory_space=pltpu.VMEM)
    hbm = pl.BlockSpec(memory_space=pl.ANY)
    dma = pltpu.SemaphoreType.DMA
    pieces = 2 * LAYERS
    gathered = pltpu.VMEM((LAYERS, NZ, NY, P_SIZE // 64, features), BF16)
    most = AHEAD + SPLIT
    blocks = pltpu.VMEM((LAYERS, 2, NT, most, 128), BF16)
    return pl.pallas_call(
        kernel,
        out_shape=jax.ShapeDtypeStruct(inputs.shape, inputs.dtype),
        in_specs=[hbm] * 5,
        out_specs=vmem,
        scratch_shapes=[
            gathered, gathered,
            pltpu.VMEM((AHEAD + rows, features), BF16),
            pltpu.VMEM(norm_gain.shape, F32),
            pltpu.VMEM(pool_scale.shape, F32),
            pltpu.VMEM((AHEAD + rows, 128), F32),
            blocks, blocks,
            pltpu.VMEM((LAYERS, 2, NT, 1, rows), F32),
            pltpu.VMEM((LAYERS, 2, most, 128), BF16),
            blocks,
            dma((pieces,)), dma((pieces, 2)),
            dma((pieces,)), dma((pieces, 3)),
            dma((LAYERS, 2)), dma((LAYERS, 2)),
            dma((LAYERS, 2)), dma((LAYERS, 2)),
            dma((LAYERS, 2)), dma((LAYERS, 2)),
            dma((1,)), dma((1,)),
            dma((4,)), dma((2, 8)),
        ],
        compiler_params=pltpu.CompilerParams(
            collective_id=0, has_side_effects=True, vmem_limit_bytes=VMEM_LIMIT
        ),
        name="mixer",
    )(inputs, norm_gain, jnp.swapaxes(in_weight, 1, 2), pool_scale, out_weight)


def solution(mesh):
    placed = (P("sp", "tp"), P(), P(None, "tp", "sp"), P(), P(None, "sp", "tp"))
    return jax.shard_map(body, mesh=mesh, in_specs=placed, out_specs=P("sp", "tp"), check_vma=False)
```

```python
import functools

import jax
import jax.numpy as jnp
from jax import lax
from jax.experimental import pallas as pl
from jax.experimental.pallas import tpu as pltpu
from jax.sharding import PartitionSpec as P

D = 4096
P_SIZE = 1024
LAYERS = 3
EPS = 1e-06
HALO = 16
AHEAD, SPLIT = 48, 112
NZ, NY, NT = 16, 4, 8
MESH = pl.DeviceIdType.MESH
BF16, F32 = jnp.bfloat16, jnp.float32


VMEM_LIMIT = 60 * 1024 * 1024
OTHERS = (4, 5, 2, 3, 6, 7, 1)
RELAYS = ((-6, (2, 1, -1)), (6, (1, -1)), (-2, (2, 1, -1)), (2, (-2, -1, 1)))
FIRST = (2, -6, -2, 6)
LATER = (1, -1, 3, -3, 4, -4, 5, -5, 7, -7, 8)
ROUND = (5,)
PLAN = {
    "start": (
        (0, 0), (5, 0), (1, 0), (0, 1), (5, 1), (2, 0), (1, 1), (0, 2), (5, 2), (3, 0), (0, 3), (2, 1), (1, 2), (5, 3), (0, 4),
    ),
    ("pre0", 0): (
        (2, 2), (3, 1), (4, 0),
    ),
    ("pool0", 0): (
        (1, 3), (5, 4),
    ),
    ("pool1", 0): (
        (5, 5), (4, 1),
    ),
    ("out0", 0): (
        (1, 4), (2, 3), (3, 2), (5, 6),
    ),
    ("in0", 1): (
        (2, 4),
    ),
    ("pre0", 1): (
        (4, 2),
    ),
    ("out1", 0): (
        (5, 7),
    ),
    ("pool0", 1): (
        (3, 3), (5, 8),
    ),
    ("pool1", 1): (
        (4, 3),
    ),
    ("out0", 1): (
        (3, 4), (5, 9),
    ),
    ("in0", 2): (
        (4, 4),
    ),
    ("out1", 1): (
        (5, 10),
    ),
}


def remote(src, dst, send, recv, sp, tp):
    return pltpu.make_async_remote_copy(
        src_ref=src, dst_ref=dst, send_sem=send, recv_sem=recv,
        device_id=(sp, tp), device_id_type=MESH,
    )


def kernel(
    x_ref, gain_ref, win_ref, scale_ref, wout_ref, out_ref,
    wi, wo, state, gain, scale, inverse, part, pair, both, rs_in, ssq, mixed, mix_in,
    z_send, z_recv, y_send, y_recv, rs_send, rs_recv,
    sq_send, sq_recv, mx_send, mx_recv, pair_send, pair_recv, px_recv, h_send, h_recv, own_sem, r_recv,
):
    sp = lax.axis_index("sp")
    t = lax.axis_index("tp")
    z, y = sp // NY, sp % NY

    def at(zz, yy):
        return ((zz + NZ) % NZ) * NY + (yy + NY) % NY

    def peer(d):
        return ((t // 2 + d // 2) % 4) * 2 + (t + d) % 2

    sp_next, sp_prev = (sp + 1) % (NZ * NY), (sp + NZ * NY - 1) % (NZ * NY)

    barrier = pltpu.get_barrier_semaphore()
    greeted = [at(z + o, y) for o in (1, -1, 2, -2, 6, -6)]
    greeted += [at(z, y + 1), at(z, y - 1), sp_next, sp_prev]
    for to in greeted:
        pl.semaphore_signal(barrier, inc=1, device_id=(to, t), device_id_type=MESH)
    for d in OTHERS:
        pl.semaphore_signal(barrier, inc=1, device_id=(sp, peer(d)), device_id_type=MESH)

    own = []
    for layer in range(LAYERS):
        own.append(pltpu.make_async_copy(win_ref.at[layer], wi.at[layer, z, y], own_sem.at[0]))
        own.append(pltpu.make_async_copy(wout_ref.at[layer], wo.at[layer, z, y], own_sem.at[0]))
    own.append(pltpu.make_async_copy(x_ref, state.at[pl.ds(AHEAD, 256)], own_sem.at[1]))
    own.append(pltpu.make_async_copy(gain_ref, gain, own_sem.at[2]))
    own.append(pltpu.make_async_copy(scale_ref, scale, own_sem.at[3]))
    for copy in own:
        copy.start()
    six = wi.at[0, pl.ds(0, 2 * LAYERS), 0]
    pltpu.make_async_copy(six, six, own_sem.at[0]).wait()
    for copy in own[2 * LAYERS:]:
        copy.wait()
    pl.semaphore_wait(barrier, len(greeted) + NT - 1)

    def piece(p):
        return (wo if p % 2 else wi).at[p // 2]

    def line(offset):
        return (z + offset + 2 * NZ) % NZ

    def along_z(p, offset, way, slot):
        block = piece(p).at[line(offset), y]
        remote(block, block, z_send.at[p], z_recv.at[p, slot], at(z + way, y), t).start()

    def along_y(p, offset, from_y, way, slot):
        block = piece(p).at[line(offset), (y + from_y + NY) % NY]
        remote(block, block, y_send.at[p], y_recv.at[p, slot], at(z, y + way), t).start()

    def landed(blocks, sem):
        remote(blocks, blocks, sem, sem, sp, t).wait_recv()

    def stage(p, k):
        if k == 0:
            for way in (6, -6, 2, -2):
                along_z(p, 0, way, 0)
            for way in (1, -1):
                along_y(p, 0, 0, way, 0)
        if k == 1:
            landed(piece(p).at[pl.ds(0, 4), 0], z_recv.at[p, 0])
            for offset, ways in RELAYS:
                for way in ways:
                    along_z(p, offset, way, 1)
            for way in (1, -1):
                for offset in FIRST:
                    along_y(p, offset, 0, way, 0)
        if k == 2:
            landed(piece(p).at[pl.ds(0, 11), 0], z_recv.at[p, 1])
            for way in (1, -1):
                for offset in LATER[:5] if way > 0 else LATER[5:]:
                    along_y(p, offset, 0, way, 1)
            for way in (1, -1):
                for offset in LATER[5:] if way > 0 else LATER[:5]:
                    along_y(p, offset, 0, way, 3)
            landed(piece(p).at[pl.ds(0, 5), pl.ds(0, 2)], y_recv.at[p, 0])
            for offset in (0, 2, -6):
                along_y(p, offset, -1, 1, 2)
            for offset in (-2, 6):
                along_y(p, offset, 1, -1, 2)
        if k == 3:
            landed(piece(p).at[pl.ds(0, 11), 0], y_recv.at[p, 1])
            for offset in LATER[:5]:
                along_y(p, offset, -1, 1, 2)
            for offset in LATER[5:]:
                along_y(p, offset, 1, -1, 2)
        if k == 4:
            landed(piece(p).at[pl.ds(0, 11), 0], y_recv.at[p, 3])
            landed(piece(p).at[:, 0], y_recv.at[p, 2])

    def ring_copy(p, way, step):
        row = piece(p).at[line(-way * step)]
        remote(
            row, row, z_send.at[p], r_recv.at[p - ROUND[0], step], at(z + way, y), t
        ).start()

    def ring_stage(p, k):
        if k == 0:
            for way in (1, -1):
                along_y(p, 0, 0, way, 0)
        if k == 1:
            landed(piece(p).at[pl.ds(0, 2), 0], y_recv.at[p, 0])
            for way in (1, -1):
                half = piece(p).at[z, (y - way + NY) % NY, :, pl.ds(128 + 128 * way, 256)]
                remote(half, half, y_send.at[p], y_recv.at[p, 1], at(z, y + way), t).start()
        if k == 2:
            landed(piece(p).at[0, 0], y_recv.at[p, 1])
        if 3 <= k <= 10:
            landed(piece(p).at[pl.ds(0, 2 if k < 10 else 1)], r_recv.at[p - ROUND[0], k - 3])
        for way, steps in ((1, 8), (-1, 7)):
            if 2 <= k < 2 + steps:
                ring_copy(p, way, k - 2)

    def advance(*where):
        for p, k in PLAN.get(where[0] if len(where) == 1 else where, ()):
            if p in ROUND:
                ring_stage(p, k)
            else:
                stage(p, k)

    ahead = remote(
        x_ref.at[pl.ds(256 - AHEAD, AHEAD)], state.at[pl.ds(0, AHEAD)],
        h_send.at[0], h_recv.at[0], sp_next, t,
    )
    ahead.start()
    window = jnp.left_shift(jnp.int32(2), t // 2)
    position = sp * 256 - AHEAD + lax.broadcasted_iota(jnp.int32, inverse.shape, 0)
    count = jnp.maximum(jnp.minimum(position + 1, window), 1)
    inverse[...] = 1.0 / count.astype(F32)
    advance("start")
    ahead.wait_recv()
    first = state[0:AHEAD].astype(F32) * (sp > 0).astype(F32)
    state[0:AHEAD] = first.astype(BF16)

    lane0 = pl.multiple_of(t * (D // NT), 128)
    lane1 = pl.multiple_of(t * 128, 128)
    group = t // 2

    def rows_in(h, layer):
        return (HALO * layer, AHEAD + SPLIT - HALO * layer) if h == 0 else (AHEAD + SPLIT, 256 - SPLIT)

    def rows_out(h, layer):
        start, count = rows_in(h, layer)
        return (start, count) if h else (start + HALO, count - HALO)

    chip, core = t // 2, t % 2
    partner = chip * 2 + 1 - core

    def same_core(dx):
        return ((chip + dx) % 4) * 2 + core

    def pair_copy(h, layer):
        rows = pl.ds(0, rows_in(h, layer)[1])
        return remote(
            part.at[layer, h, 1 - core, :, rows], pair.at[layer, h, :, rows],
            pair_send.at[layer, h], pair_recv.at[layer, h], sp, partner,
        )

    def sum_copy(h, layer, dx):
        rows = pl.ds(0, rows_in(h, layer)[1])
        return remote(
            both.at[layer, h, dx, rows], rs_in.at[layer, h, dx, rows],
            rs_send.at[layer, h], rs_recv.at[layer, h], sp, same_core(dx),
        )

    def square_copy(h, layer, d, j):
        return remote(
            ssq.at[layer, h, t], ssq.at[layer, h, t],
            sq_send.at[layer, h], sq_recv.at[layer, h], sp, j,
        )

    def mixed_copy(h, layer, j, recv):
        rows = pl.ds(0, rows_out(h, layer)[1])
        return remote(
            mixed.at[layer, h, rows], mix_in.at[layer, h, t, rows],
            mx_send.at[layer, h], recv.at[layer, h], sp, j,
        )

    def project_in(h, layer):
        start, count = rows_in(h, layer)
        wide = state[start:start + count].astype(F32)
        squares = jnp.sum(wide * wide, axis=1, keepdims=True)
        squares = jnp.broadcast_to(squares, (count, 128))
        squares = jnp.concatenate([squares, jnp.zeros((256 - count, 128), F32)], axis=0)
        ssq[layer, h, t] = squares.T[0:1, :]
        for d in OTHERS:
            square_copy(h, layer, d, peer(d)).start()
        own_gain = gain[pl.ds(layer, 1), pl.ds(lane0, D // NT)]
        scaled = (wide * own_gain).astype(BF16)
        weights = wi[layer].reshape(P_SIZE, D // NT)
        partial = lax.dot_general(
            scaled, weights, (((1,), (1,)), ((), ())), preferred_element_type=F32
        ).astype(BF16)
        for j in range(NT):
            part[layer, h, j % 2, j // 2, 0:count] = partial[:, j * 128:(j + 1) * 128]
        pair_copy(h, layer).start()

    def chip_sum(h, layer, to):
        count = rows_in(h, layer)[1]
        own = part[layer, h, core, to, 0:count].astype(F32)
        return own + pair[layer, h, to, 0:count].astype(F32)

    def combine(h, layer):
        count = rows_in(h, layer)[1]
        landed(pair.at[layer, h, :, pl.ds(0, count)], pair_recv.at[layer, h])
        for dx in (2, 1, 3):
            total = chip_sum(h, layer, (chip + dx) % 4)
            both[layer, h, dx, 0:count] = total.astype(BF16)
            sum_copy(h, layer, dx).start()

    def pool(h, layer, tail):
        count = rows_in(h, layer)[1]
        start, out_count = rows_out(h, layer)
        seven = pl.ds(0, NT - 1)
        landed(ssq.at[layer, h, seven], sq_recv.at[layer, h])
        inv_rms = lax.rsqrt(jnp.sum(ssq[layer, h], axis=0) / D + EPS)
        inv_rms = jnp.broadcast_to(inv_rms, (128, 256)).T[0:count]
        total = chip_sum(h, layer, chip)
        landed(rs_in.at[layer, h, pl.ds(0, 3), pl.ds(0, count)], rs_recv.at[layer, h])
        for dx in (1, 2, 3):
            total = total + rs_in[layer, h, dx, 0:count].astype(F32)
        pool_in = (total * inv_rms).astype(BF16).astype(F32)
        run = pool_in if tail is None else jnp.concatenate([tail, pool_in], axis=0)
        own = run[HALO:]
        picked = None
        for g in range(4):
            run = run + pltpu.roll(run, 1 << g, 0)
            picked = run if g == 0 else jnp.where(group >= g, run, picked)
        means = picked[HALO:] * inverse[start:start + out_count] - own
        own_scale = scale[pl.ds(layer, 1), pl.ds(lane1, 128)]
        mixed[layer, h, 0:out_count] = (means * own_scale).astype(BF16)
        for dx in (2, 1, 3):
            mixed_copy(h, layer, same_core(dx), mx_recv).start()
        mixed_copy(h, layer, partner, px_recv).start()
        mix_in[layer, h, t, 0:out_count] = mixed[layer, h, 0:out_count]
        return pool_in[count - HALO:]

    def relay(h, layer):
        rows = pl.ds(0, rows_out(h, layer)[1])
        landed(mix_in.at[layer, h, pl.ds(0, 3), rows], mx_recv.at[layer, h])
        for dx in (1, 2, 3):
            block = mix_in.at[layer, h, same_core(dx), rows]
            remote(
                block, block, mx_send.at[layer, h], px_recv.at[layer, h], sp, partner
            ).start()

    def project_out(h, layer):
        start, count = rows_out(h, layer)
        landed(mix_in.at[layer, h, pl.ds(0, 4), pl.ds(0, count)], px_recv.at[layer, h])
        pooled = jnp.concatenate(
            [mix_in[layer, h, k, 0:count] for k in range(NT)], axis=1
        )
        branch = jnp.dot(
            pooled, wo[layer].reshape(P_SIZE, D // NT), preferred_element_type=F32
        )
        after = (state[start:start + count].astype(F32) + branch).astype(BF16)
        if layer == LAYERS - 1:
            out_ref[start - AHEAD:start - AHEAD + count] = after
        else:
            state[start:start + count] = after

    project_in(0, 0)
    advance("pre0", 0)
    combine(0, 0)
    project_in(1, 0)
    combine(1, 0)
    for layer in range(LAYERS):
        advance("pool0", layer)
        tail = pool(0, layer, None)
        advance("pool1", layer)
        pool(1, layer, tail)
        advance("out0", layer)
        relay(0, layer)
        project_out(0, layer)
        if layer < LAYERS - 1:
            advance("in0", layer + 1)
            project_in(0, layer + 1)
            advance("pre0", layer + 1)
            combine(0, layer + 1)
        advance("out1", layer)
        relay(1, layer)
        project_out(1, layer)
        if layer < LAYERS - 1:
            project_in(1, layer + 1)
            combine(1, layer + 1)

    def left(blocks, sem):
        remote(blocks, blocks, sem, sem, sp, t).wait_send()

    ahead.wait_send()
    for p in range(2 * LAYERS):
        if p in ROUND:
            left(piece(p).at[pl.ds(0, 15)], z_send.at[p])
            left(piece(p).at[pl.ds(0, 3), 0], y_send.at[p])
        else:
            left(piece(p).at[pl.ds(0, 15), 0], z_send.at[p])
            left(piece(p).at[pl.ds(0, 12)], y_send.at[p])
    seven = pl.ds(0, NT - 1)
    for layer in range(LAYERS):
        for h in (0, 1):
            count, out_count = rows_in(h, layer)[1], rows_out(h, layer)[1]
            left(ssq.at[layer, h, seven], sq_send.at[layer, h])
            left(pair.at[layer, h, :, pl.ds(0, count)], pair_send.at[layer, h])
            left(both.at[layer, h, pl.ds(0, 3), pl.ds(0, count)], rs_send.at[layer, h])
            left(mix_in.at[layer, h, seven, pl.ds(0, out_count)], mx_send.at[layer, h])


def body(inputs, norm_gain, in_weight, pool_scale, out_weight):
    rows, features = inputs.shape
    vmem = pl.BlockSpec(memory_space=pltpu.VMEM)
    hbm = pl.BlockSpec(memory_space=pl.ANY)
    dma = pltpu.SemaphoreType.DMA
    pieces = 2 * LAYERS
    gathered = pltpu.VMEM((LAYERS, NZ, NY, P_SIZE // 64, features), BF16)
    most = AHEAD + SPLIT
    blocks = pltpu.VMEM((LAYERS, 2, NT, most, 128), BF16)
    quarter = pltpu.VMEM((LAYERS, 2, 4, most, 128), BF16)
    return pl.pallas_call(
        kernel,
        out_shape=jax.ShapeDtypeStruct(inputs.shape, inputs.dtype),
        in_specs=[hbm] * 5,
        out_specs=vmem,
        scratch_shapes=[
            gathered, gathered,
            pltpu.VMEM((AHEAD + rows, features), BF16),
            pltpu.VMEM(norm_gain.shape, F32),
            pltpu.VMEM(pool_scale.shape, F32),
            pltpu.VMEM((AHEAD + rows, 128), F32),
            pltpu.VMEM((LAYERS, 2, 2, 4, most, 128), BF16),
            quarter, quarter, quarter,
            pltpu.VMEM((LAYERS, 2, NT, 1, rows), F32),
            pltpu.VMEM((LAYERS, 2, most, 128), BF16),
            blocks,
            dma((pieces,)), dma((pieces, 2)),
            dma((pieces,)), dma((pieces, 4)),
            dma((LAYERS, 2)), dma((LAYERS, 2)),
            dma((LAYERS, 2)), dma((LAYERS, 2)),
            dma((LAYERS, 2)), dma((LAYERS, 2)),
            dma((LAYERS, 2)), dma((LAYERS, 2)), dma((LAYERS, 2)),
            dma((1,)), dma((1,)),
            dma((4,)), dma((2, 8)),
        ],
        compiler_params=pltpu.CompilerParams(
            collective_id=0, has_side_effects=True, vmem_limit_bytes=VMEM_LIMIT
        ),
        name="mixer",
    )(inputs, norm_gain, jnp.swapaxes(in_weight, 1, 2), pool_scale, out_weight)


def solution(mesh):
    placed = (P("sp", "tp"), P(), P(None, "tp", "sp"), P(), P(None, "sp", "tp"))
    return jax.shard_map(body, mesh=mesh, in_specs=placed, out_specs=P("sp", "tp"), check_vma=False)
```

```python
import functools

import jax
import jax.numpy as jnp
from jax import lax
from jax.experimental import pallas as pl
from jax.experimental.pallas import tpu as pltpu
from jax.sharding import PartitionSpec as P

D = 4096
P_SIZE = 1024
LAYERS = 3
EPS = 1e-06
HALO = 16
AHEAD, SPLIT = 48, 128
NZ, NY, NT = 16, 4, 8
MESH = pl.DeviceIdType.MESH
BF16, F32 = jnp.bfloat16, jnp.float32


VMEM_LIMIT = 60 * 1024 * 1024
OTHERS = (4, 5, 2, 3, 6, 7, 1)
RELAYS = ((-6, (2, 1, -1)), (6, (1, -1)), (-2, (2, 1, -1)), (2, (-2, -1, 1)))
FIRST = (2, -6, -2, 6)
LATER = (1, -1, 3, -3, 4, -4, 5, -5, 7, -7, 8)
ROUND = (5,)
PLAN = {
    "start": (
        (0, 0), (5, 0), (1, 0), (0, 1), (5, 1), (2, 0), (1, 1), (0, 2), (5, 2), (3, 0), (0, 3), (2, 1), (1, 2), (4, 0), (5, 3), (0, 4),
    ),
    ("pre0", 0): (
        (2, 2), (3, 1),
    ),
    ("pool0", 0): (
        (1, 3), (5, 4),
    ),
    ("pool1", 0): (
        (5, 5), (4, 1),
    ),
    ("out0", 0): (
        (1, 4), (2, 3), (3, 2), (5, 6),
    ),
    ("in0", 1): (
        (2, 4),
    ),
    ("pre0", 1): (
        (4, 2),
    ),
    ("out1", 0): (
        (5, 7),
    ),
    ("pool0", 1): (
        (3, 3), (5, 8),
    ),
    ("pool1", 1): (
        (4, 3),
    ),
    ("out0", 1): (
        (3, 4), (5, 9),
    ),
    ("in0", 2): (
        (4, 4),
    ),
    ("out1", 1): (
        (5, 10),
    ),
}


def remote(src, dst, send, recv, sp, tp):
    return pltpu.make_async_remote_copy(
        src_ref=src, dst_ref=dst, send_sem=send, recv_sem=recv,
        device_id=(sp, tp), device_id_type=MESH,
    )


def kernel(
    x_ref, gain_ref, win_ref, scale_ref, wout_ref, out_ref,
    wi, wo, state, gain, scale, inverse, part, pair, both, rs_in, ssq, mixed, mix_in,
    z_send, z_recv, y_send, y_recv, rs_send, rs_recv,
    sq_send, sq_recv, mx_send, mx_recv, pair_send, pair_recv, px_recv, h_send, h_recv, own_sem, r_recv,
):
    sp = lax.axis_index("sp")
    t = lax.axis_index("tp")
    z, y = sp // NY, sp % NY

    def at(zz, yy):
        return ((zz + NZ) % NZ) * NY + (yy + NY) % NY

    def peer(d):
        return ((t // 2 + d // 2) % 4) * 2 + (t + d) % 2

    sp_next, sp_prev = (sp + 1) % (NZ * NY), (sp + NZ * NY - 1) % (NZ * NY)

    barrier = pltpu.get_barrier_semaphore()
    greeted = [at(z + o, y) for o in (1, -1, 2, -2, 6, -6)]
    greeted += [at(z, y + 1), at(z, y - 1), sp_next, sp_prev]
    for to in greeted:
        pl.semaphore_signal(barrier, inc=1, device_id=(to, t), device_id_type=MESH)
    for d in OTHERS:
        pl.semaphore_signal(barrier, inc=1, device_id=(sp, peer(d)), device_id_type=MESH)

    own = []
    for layer in range(LAYERS):
        own.append(pltpu.make_async_copy(win_ref.at[layer], wi.at[layer, z, y], own_sem.at[0]))
        own.append(pltpu.make_async_copy(wout_ref.at[layer], wo.at[layer, z, y], own_sem.at[0]))
    own.append(pltpu.make_async_copy(x_ref, state.at[pl.ds(AHEAD, 256)], own_sem.at[1]))
    own.append(pltpu.make_async_copy(gain_ref, gain, own_sem.at[2]))
    own.append(pltpu.make_async_copy(scale_ref, scale, own_sem.at[3]))
    for copy in own:
        copy.start()
    six = wi.at[0, pl.ds(0, 2 * LAYERS), 0]
    pltpu.make_async_copy(six, six, own_sem.at[0]).wait()
    for copy in own[2 * LAYERS:]:
        copy.wait()
    pl.semaphore_wait(barrier, len(greeted) + NT - 1)

    def piece(p):
        return (wo if p % 2 else wi).at[p // 2]

    def line(offset):
        return (z + offset + 2 * NZ) % NZ

    def along_z(p, offset, way, slot):
        block = piece(p).at[line(offset), y]
        remote(block, block, z_send.at[p], z_recv.at[p, slot], at(z + way, y), t).start()

    def along_y(p, offset, from_y, way, slot):
        block = piece(p).at[line(offset), (y + from_y + NY) % NY]
        remote(block, block, y_send.at[p], y_recv.at[p, slot], at(z, y + way), t).start()

    def landed(blocks, sem):
        remote(blocks, blocks, sem, sem, sp, t).wait_recv()

    def stage(p, k):
        if k == 0:
            for way in (6, -6, 2, -2):
                along_z(p, 0, way, 0)
            for way in (1, -1):
                along_y(p, 0, 0, way, 0)
        if k == 1:
            landed(piece(p).at[pl.ds(0, 4), 0], z_recv.at[p, 0])
            for offset, ways in RELAYS:
                for way in ways:
                    along_z(p, offset, way, 1)
            for way in (1, -1):
                for offset in FIRST:
                    along_y(p, offset, 0, way, 0)
        if k == 2:
            landed(piece(p).at[pl.ds(0, 11), 0], z_recv.at[p, 1])
            for way in (1, -1):
                for offset in LATER[:5] if way > 0 else LATER[5:]:
                    along_y(p, offset, 0, way, 1)
            for way in (1, -1):
                for offset in LATER[5:] if way > 0 else LATER[:5]:
                    along_y(p, offset, 0, way, 3)
            landed(piece(p).at[pl.ds(0, 5), pl.ds(0, 2)], y_recv.at[p, 0])
            for offset in (0, 2, -6):
                along_y(p, offset, -1, 1, 2)
            for offset in (-2, 6):
                along_y(p, offset, 1, -1, 2)
        if k == 3:
            landed(piece(p).at[pl.ds(0, 11), 0], y_recv.at[p, 1])
            for offset in LATER[:5]:
                along_y(p, offset, -1, 1, 2)
            for offset in LATER[5:]:
                along_y(p, offset, 1, -1, 2)
        if k == 4:
            landed(piece(p).at[pl.ds(0, 11), 0], y_recv.at[p, 3])
            landed(piece(p).at[:, 0], y_recv.at[p, 2])

    def ring_copy(p, way, step):
        row = piece(p).at[line(-way * step)]
        remote(
            row, row, z_send.at[p], r_recv.at[p - ROUND[0], step], at(z + way, y), t
        ).start()

    def ring_stage(p, k):
        if k == 0:
            for way in (1, -1):
                along_y(p, 0, 0, way, 0)
        if k == 1:
            landed(piece(p).at[pl.ds(0, 2), 0], y_recv.at[p, 0])
            for way in (1, -1):
                half = piece(p).at[z, (y - way + NY) % NY, :, pl.ds(128 + 128 * way, 256)]
                remote(half, half, y_send.at[p], y_recv.at[p, 1], at(z, y + way), t).start()
        if k == 2:
            landed(piece(p).at[0, 0], y_recv.at[p, 1])
        if 3 <= k <= 10:
            landed(piece(p).at[pl.ds(0, 2 if k < 10 else 1)], r_recv.at[p - ROUND[0], k - 3])
        for way, steps in ((1, 8), (-1, 7)):
            if 2 <= k < 2 + steps:
                ring_copy(p, way, k - 2)

    def advance(*where):
        for p, k in PLAN.get(where[0] if len(where) == 1 else where, ()):
            if p in ROUND:
                ring_stage(p, k)
            else:
                stage(p, k)

    ahead = remote(
        x_ref.at[pl.ds(256 - AHEAD, AHEAD)], state.at[pl.ds(0, AHEAD)],
        h_send.at[0], h_recv.at[0], sp_next, t,
    )
    ahead.start()
    window = jnp.left_shift(jnp.int32(2), t // 2)
    position = sp * 256 - AHEAD + lax.broadcasted_iota(jnp.int32, inverse.shape, 0)
    count = jnp.maximum(jnp.minimum(position + 1, window), 1)
    inverse[...] = 1.0 / count.astype(F32)
    advance("start")
    ahead.wait_recv()
    first = state[0:AHEAD].astype(F32) * (sp > 0).astype(F32)
    state[0:AHEAD] = first.astype(BF16)

    lane0 = pl.multiple_of(t * (D // NT), 128)
    lane1 = pl.multiple_of(t * 128, 128)
    group = t // 2

    def rows_in(h, layer):
        return (HALO * layer, AHEAD + SPLIT - HALO * layer) if h == 0 else (AHEAD + SPLIT, 256 - SPLIT)

    def rows_out(h, layer):
        start, count = rows_in(h, layer)
        return (start, count) if h else (start + HALO, count - HALO)

    chip, core = t // 2, t % 2
    partner = chip * 2 + 1 - core

    def same_core(dx):
        return ((chip + dx) % 4) * 2 + core

    def pair_copy(h, layer):
        rows = pl.ds(0, rows_in(h, layer)[1])
        return remote(
            part.at[layer, h, 1 - core, :, rows], pair.at[layer, h, :, rows],
            pair_send.at[layer, h], pair_recv.at[layer, h], sp, partner,
        )

    def sum_copy(h, layer, dx):
        rows = pl.ds(0, rows_in(h, layer)[1])
        return remote(
            both.at[layer, h, dx, rows], rs_in.at[layer, h, dx, rows],
            rs_send.at[layer, h], rs_recv.at[layer, h], sp, same_core(dx),
        )

    def square_copy(h, layer, d, j):
        return remote(
            ssq.at[layer, h, t], ssq.at[layer, h, t],
            sq_send.at[layer, h], sq_recv.at[layer, h], sp, j,
        )

    def mixed_copy(h, layer, j, recv):
        rows = pl.ds(0, rows_out(h, layer)[1])
        return remote(
            mixed.at[layer, h, rows], mix_in.at[layer, h, t, rows],
            mx_send.at[layer, h], recv.at[layer, h], sp, j,
        )

    def project_in(h, layer):
        start, count = rows_in(h, layer)
        wide = state[start:start + count].astype(F32)
        own_gain = gain[pl.ds(layer, 1), pl.ds(lane0, D // NT)]
        scaled = (wide * own_gain).astype(BF16)
        weights = wi[layer].reshape(P_SIZE, D // NT)
        partial = lax.dot_general(
            scaled, weights, (((1,), (1,)), ((), ())), preferred_element_type=F32
        ).astype(BF16)
        for j in range(NT):
            part[layer, h, j % 2, j // 2, 0:count] = partial[:, j * 128:(j + 1) * 128]
        pair_copy(h, layer).start()
        squares = jnp.sum(wide * wide, axis=1, keepdims=True)
        squares = jnp.broadcast_to(squares, (count, 128))
        squares = jnp.concatenate([squares, jnp.zeros((256 - count, 128), F32)], axis=0)
        ssq[layer, h, t] = squares.T[0:1, :]
        for d in OTHERS:
            square_copy(h, layer, d, peer(d)).start()

    def chip_sum(h, layer, to):
        count = rows_in(h, layer)[1]
        own = part[layer, h, core, to, 0:count].astype(F32)
        return own + pair[layer, h, to, 0:count].astype(F32)

    def combine(h, layer):
        count = rows_in(h, layer)[1]
        landed(pair.at[layer, h, :, pl.ds(0, count)], pair_recv.at[layer, h])
        for dx in (2, 1, 3):
            total = chip_sum(h, layer, (chip + dx) % 4)
            both[layer, h, dx, 0:count] = total.astype(BF16)
            sum_copy(h, layer, dx).start()

    def pool(h, layer, tail):
        count = rows_in(h, layer)[1]
        start, out_count = rows_out(h, layer)
        seven = pl.ds(0, NT - 1)
        landed(ssq.at[layer, h, seven], sq_recv.at[layer, h])
        inv_rms = lax.rsqrt(jnp.sum(ssq[layer, h], axis=0) / D + EPS)
        inv_rms = jnp.broadcast_to(inv_rms, (128, 256)).T[0:count]
        total = chip_sum(h, layer, chip)
        landed(rs_in.at[layer, h, pl.ds(0, 3), pl.ds(0, count)], rs_recv.at[layer, h])
        for dx in (1, 2, 3):
            total = total + rs_in[layer, h, dx, 0:count].astype(F32)
        pool_in = (total * inv_rms).astype(BF16).astype(F32)
        run = pool_in if tail is None else jnp.concatenate([tail, pool_in], axis=0)
        own = run[HALO:]
        picked = None
        for g in range(4):
            run = run + pltpu.roll(run, 1 << g, 0)
            picked = run if g == 0 else jnp.where(group >= g, run, picked)
        means = picked[HALO:] * inverse[start:start + out_count] - own
        own_scale = scale[pl.ds(layer, 1), pl.ds(lane1, 128)]
        mixed[layer, h, 0:out_count] = (means * own_scale).astype(BF16)
        for dx in (2, 1, 3):
            mixed_copy(h, layer, same_core(dx), mx_recv).start()
        mixed_copy(h, layer, partner, px_recv).start()
        mix_in[layer, h, t, 0:out_count] = mixed[layer, h, 0:out_count]
        return pool_in[count - HALO:]

    def relay(h, layer):
        rows = pl.ds(0, rows_out(h, layer)[1])
        landed(mix_in.at[layer, h, pl.ds(0, 3), rows], mx_recv.at[layer, h])
        for dx in (1, 2, 3):
            block = mix_in.at[layer, h, same_core(dx), rows]
            remote(
                block, block, mx_send.at[layer, h], px_recv.at[layer, h], sp, partner
            ).start()

    def project_out(h, layer):
        start, count = rows_out(h, layer)
        landed(mix_in.at[layer, h, pl.ds(0, 4), pl.ds(0, count)], px_recv.at[layer, h])
        pooled = jnp.concatenate(
            [mix_in[layer, h, k, 0:count] for k in range(NT)], axis=1
        )
        branch = jnp.dot(
            pooled, wo[layer].reshape(P_SIZE, D // NT), preferred_element_type=F32
        )
        after = (state[start:start + count].astype(F32) + branch).astype(BF16)
        if layer == LAYERS - 1:
            out_ref[start - AHEAD:start - AHEAD + count] = after
        else:
            state[start:start + count] = after

    project_in(0, 0)
    advance("pre0", 0)
    combine(0, 0)
    project_in(1, 0)
    combine(1, 0)
    for layer in range(LAYERS):
        advance("pool0", layer)
        tail = pool(0, layer, None)
        advance("pool1", layer)
        pool(1, layer, tail)
        advance("out0", layer)
        relay(0, layer)
        project_out(0, layer)
        if layer < LAYERS - 1:
            advance("in0", layer + 1)
            project_in(0, layer + 1)
            advance("pre0", layer + 1)
            combine(0, layer + 1)
        advance("out1", layer)
        relay(1, layer)
        project_out(1, layer)
        if layer < LAYERS - 1:
            project_in(1, layer + 1)
            combine(1, layer + 1)

    def left(blocks, sem):
        remote(blocks, blocks, sem, sem, sp, t).wait_send()

    ahead.wait_send()
    for p in range(2 * LAYERS):
        if p in ROUND:
            left(piece(p).at[pl.ds(0, 15)], z_send.at[p])
            left(piece(p).at[pl.ds(0, 3), 0], y_send.at[p])
        else:
            left(piece(p).at[pl.ds(0, 15), 0], z_send.at[p])
            left(piece(p).at[pl.ds(0, 12)], y_send.at[p])
    seven = pl.ds(0, NT - 1)
    for layer in range(LAYERS):
        for h in (0, 1):
            count, out_count = rows_in(h, layer)[1], rows_out(h, layer)[1]
            left(ssq.at[layer, h, seven], sq_send.at[layer, h])
            left(pair.at[layer, h, :, pl.ds(0, count)], pair_send.at[layer, h])
            left(both.at[layer, h, pl.ds(0, 3), pl.ds(0, count)], rs_send.at[layer, h])
            left(mix_in.at[layer, h, seven, pl.ds(0, out_count)], mx_send.at[layer, h])


def body(inputs, norm_gain, in_weight, pool_scale, out_weight):
    rows, features = inputs.shape
    vmem = pl.BlockSpec(memory_space=pltpu.VMEM)
    hbm = pl.BlockSpec(memory_space=pl.ANY)
    dma = pltpu.SemaphoreType.DMA
    pieces = 2 * LAYERS
    gathered = pltpu.VMEM((LAYERS, NZ, NY, P_SIZE // 64, features), BF16)
    most = AHEAD + SPLIT
    blocks = pltpu.VMEM((LAYERS, 2, NT, most, 128), BF16)
    quarter = pltpu.VMEM((LAYERS, 2, 4, most, 128), BF16)
    return pl.pallas_call(
        kernel,
        out_shape=jax.ShapeDtypeStruct(inputs.shape, inputs.dtype),
        in_specs=[hbm] * 5,
        out_specs=vmem,
        scratch_shapes=[
            gathered, gathered,
            pltpu.VMEM((AHEAD + rows, features), BF16),
            pltpu.VMEM(norm_gain.shape, F32),
            pltpu.VMEM(pool_scale.shape, F32),
            pltpu.VMEM((AHEAD + rows, 128), F32),
            pltpu.VMEM((LAYERS, 2, 2, 4, most, 128), BF16),
            quarter, quarter, quarter,
            pltpu.VMEM((LAYERS, 2, NT, 1, rows), F32),
            pltpu.VMEM((LAYERS, 2, most, 128), BF16),
            blocks,
            dma((pieces,)), dma((pieces, 2)),
            dma((pieces,)), dma((pieces, 4)),
            dma((LAYERS, 2)), dma((LAYERS, 2)),
            dma((LAYERS, 2)), dma((LAYERS, 2)),
            dma((LAYERS, 2)), dma((LAYERS, 2)),
            dma((LAYERS, 2)), dma((LAYERS, 2)), dma((LAYERS, 2)),
            dma((1,)), dma((1,)),
            dma((4,)), dma((2, 8)),
        ],
        compiler_params=pltpu.CompilerParams(
            collective_id=0, has_side_effects=True, vmem_limit_bytes=VMEM_LIMIT
        ),
        name="mixer",
    )(inputs, norm_gain, jnp.swapaxes(in_weight, 1, 2), pool_scale, out_weight)


def solution(mesh):
    placed = (P("sp", "tp"), P(), P(None, "tp", "sp"), P(), P(None, "sp", "tp"))
    return jax.shard_map(body, mesh=mesh, in_specs=placed, out_specs=P("sp", "tp"), check_vma=False)
```

```python
import functools

import jax
import jax.numpy as jnp
from jax import lax
from jax.experimental import pallas as pl
from jax.experimental.pallas import tpu as pltpu
from jax.sharding import PartitionSpec as P

D = 4096
P_SIZE = 1024
LAYERS = 3
EPS = 1e-06
HALO = 16
AHEAD, SPLIT = 48, 128
NZ, NY, NT = 16, 4, 8
MESH = pl.DeviceIdType.MESH
BF16, F32 = jnp.bfloat16, jnp.float32


VMEM_LIMIT = 60 * 1024 * 1024
OTHERS = (4, 5, 2, 3, 6, 7, 1)
RELAYS = ((-6, (2, 1, -1)), (6, (1, -1)), (-2, (2, 1, -1)), (2, (-2, -1, 1)))
FIRST = (2, -6, -2, 6)
LATER = (1, -1, 3, -3, 4, -4, 5, -5, 7, -7, 8)
ROUND = (5,)
PLAN = {
    "start": (
        (0, 0), (5, 0), (1, 0), (0, 1), (5, 1), (2, 0), (1, 1), (0, 2), (5, 2), (3, 0), (0, 3), (2, 1), (1, 2), (4, 0), (5, 3), (0, 4),
    ),
    ("pre0", 0): (
        (1, 3, 1), (2, 2), (3, 1),
    ),
    ("pool0", 0): (
        (1, 3, 0), (5, 4),
    ),
    ("pool1", 0): (
        (5, 5), (4, 1),
    ),
    ("out0", 0): (
        (1, 4), (3, 2), (5, 6),
    ),
    ("in0", 1): (
        (2, 4),
    ),
    ("pre0", 1): (
        (4, 2),
    ),
    ("out1", 0): (
        (5, 7),
    ),
    ("pool0", 1): (
        (3, 3), (5, 8),
    ),
    ("pool1", 1): (
        (4, 3),
    ),
    ("out0", 1): (
        (3, 4), (5, 9),
    ),
    ("in0", 2): (
        (4, 4),
    ),
    ("out1", 1): (
        (5, 10),
    ),
    ("pass0", 0): (
        (2, 3),
    ),
}


def remote(src, dst, send, recv, sp, tp):
    return pltpu.make_async_remote_copy(
        src_ref=src, dst_ref=dst, send_sem=send, recv_sem=recv,
        device_id=(sp, tp), device_id_type=MESH,
    )


def kernel(
    x_ref, gain_ref, win_ref, scale_ref, wout_ref, out_ref,
    wi, wo, state, gain, scale, inverse, part, pair, both, rs_in, ssq, mixed, mix_in,
    z_send, z_recv, y_send, y_recv, rs_send, rs_recv,
    sq_send, sq_recv, mx_send, mx_recv, pair_send, pair_recv, px_recv, h_send, h_recv, own_sem, r_recv,
):
    sp = lax.axis_index("sp")
    t = lax.axis_index("tp")
    z, y = sp // NY, sp % NY

    def at(zz, yy):
        return ((zz + NZ) % NZ) * NY + (yy + NY) % NY

    def peer(d):
        return ((t // 2 + d // 2) % 4) * 2 + (t + d) % 2

    sp_next, sp_prev = (sp + 1) % (NZ * NY), (sp + NZ * NY - 1) % (NZ * NY)

    barrier = pltpu.get_barrier_semaphore()
    greeted = [at(z + o, y) for o in (1, -1, 2, -2, 6, -6)]
    greeted += [at(z, y + 1), at(z, y - 1), sp_next, sp_prev]
    for to in greeted:
        pl.semaphore_signal(barrier, inc=1, device_id=(to, t), device_id_type=MESH)
    for d in OTHERS:
        pl.semaphore_signal(barrier, inc=1, device_id=(sp, peer(d)), device_id_type=MESH)

    own = []
    for layer in range(LAYERS):
        own.append(pltpu.make_async_copy(win_ref.at[layer], wi.at[layer, z, y], own_sem.at[0]))
        own.append(pltpu.make_async_copy(wout_ref.at[layer], wo.at[layer, z, y], own_sem.at[0]))
    own.append(pltpu.make_async_copy(x_ref, state.at[pl.ds(AHEAD, 256)], own_sem.at[1]))
    own.append(pltpu.make_async_copy(gain_ref, gain, own_sem.at[2]))
    own.append(pltpu.make_async_copy(scale_ref, scale, own_sem.at[3]))
    for copy in own:
        copy.start()
    six = wi.at[0, pl.ds(0, 2 * LAYERS), 0]
    pltpu.make_async_copy(six, six, own_sem.at[0]).wait()
    for copy in own[2 * LAYERS:]:
        copy.wait()
    pl.semaphore_wait(barrier, len(greeted) + NT - 1)

    def piece(p):
        return (wo if p % 2 else wi).at[p // 2]

    def line(offset):
        return (z + offset + 2 * NZ) % NZ

    def along_z(p, offset, way, slot):
        block = piece(p).at[line(offset), y]
        remote(block, block, z_send.at[p], z_recv.at[p, slot], at(z + way, y), t).start()

    def along_y(p, offset, from_y, way, slot):
        block = piece(p).at[line(offset), (y + from_y + NY) % NY]
        remote(block, block, y_send.at[p], y_recv.at[p, slot], at(z, y + way), t).start()

    def landed(blocks, sem):
        remote(blocks, blocks, sem, sem, sp, t).wait_recv()

    def stage(p, k):
        if k == 0:
            for way in (6, -6, 2, -2):
                along_z(p, 0, way, 0)
            for way in (1, -1):
                along_y(p, 0, 0, way, 0)
        if k == 1:
            landed(piece(p).at[pl.ds(0, 4), 0], z_recv.at[p, 0])
            for offset, ways in RELAYS:
                for way in ways:
                    along_z(p, offset, way, 1)
            for way in (1, -1):
                for offset in FIRST:
                    along_y(p, offset, 0, way, 0)
        if k == 2:
            landed(piece(p).at[pl.ds(0, 11), 0], z_recv.at[p, 1])
            for way in (1, -1):
                for offset in LATER[:5] if way > 0 else LATER[5:]:
                    along_y(p, offset, 0, way, 1)
            for way in (1, -1):
                for offset in LATER[5:] if way > 0 else LATER[:5]:
                    along_y(p, offset, 0, way, 3)
            landed(piece(p).at[pl.ds(0, 5), pl.ds(0, 2)], y_recv.at[p, 0])
            for offset in (0, 2, -6):
                along_y(p, offset, -1, 1, 2)
            for offset in (-2, 6):
                along_y(p, offset, 1, -1, 2)
        if k == 3:
            landed(piece(p).at[pl.ds(0, 11), 0], y_recv.at[p, 1])
            for offset in LATER[:5]:
                along_y(p, offset, -1, 1, 2)
            for offset in LATER[5:]:
                along_y(p, offset, 1, -1, 2)
        if k == 4:
            landed(piece(p).at[pl.ds(0, 11), 0], y_recv.at[p, 3])
            landed(piece(p).at[:, 0], y_recv.at[p, 2])

    def ring_copy(p, way, step):
        row = piece(p).at[line(-way * step)]
        remote(
            row, row, z_send.at[p], r_recv.at[p - ROUND[0], step], at(z + way, y), t
        ).start()

    def ring_stage(p, k):
        if k == 0:
            for way in (1, -1):
                along_y(p, 0, 0, way, 0)
        if k == 1:
            landed(piece(p).at[pl.ds(0, 2), 0], y_recv.at[p, 0])
            for way in (1, -1):
                half = piece(p).at[z, (y - way + NY) % NY, :, pl.ds(128 + 128 * way, 256)]
                remote(half, half, y_send.at[p], y_recv.at[p, 1], at(z, y + way), t).start()
        if k == 2:
            landed(piece(p).at[0, 0], y_recv.at[p, 1])
        if 3 <= k <= 10:
            landed(piece(p).at[pl.ds(0, 2 if k < 10 else 1)], r_recv.at[p - ROUND[0], k - 3])
        for way, steps in ((1, 8), (-1, 7)):
            if 2 <= k < 2 + steps:
                ring_copy(p, way, k - 2)

    def advance(*where):
        for p, k, *only in PLAN.get(where[0] if len(where) == 1 else where, ()):
            run = functools.partial(ring_stage if p in ROUND else stage, p, k)
            if only:
                pl.when(t % 2 == only[0])(run)
            else:
                run()

    ahead = remote(
        x_ref.at[pl.ds(256 - AHEAD, AHEAD)], state.at[pl.ds(0, AHEAD)],
        h_send.at[0], h_recv.at[0], sp_next, t,
    )
    ahead.start()
    window = jnp.left_shift(jnp.int32(2), t // 2)
    position = sp * 256 - AHEAD + lax.broadcasted_iota(jnp.int32, inverse.shape, 0)
    count = jnp.maximum(jnp.minimum(position + 1, window), 1)
    inverse[...] = 1.0 / count.astype(F32)
    advance("start")
    ahead.wait_recv()
    first = state[0:AHEAD].astype(F32) * (sp > 0).astype(F32)
    state[0:AHEAD] = first.astype(BF16)

    lane0 = pl.multiple_of(t * (D // NT), 128)
    lane1 = pl.multiple_of(t * 128, 128)
    group = t // 2

    def rows_in(h, layer):
        return (HALO * layer, AHEAD + SPLIT - HALO * layer) if h == 0 else (AHEAD + SPLIT, 256 - SPLIT)

    def rows_out(h, layer):
        start, count = rows_in(h, layer)
        return (start, count) if h else (start + HALO, count - HALO)

    chip, core = t // 2, t % 2
    partner = chip * 2 + 1 - core

    def same_core(dx):
        return ((chip + dx) % 4) * 2 + core

    def pair_copy(h, layer):
        rows = pl.ds(0, rows_in(h, layer)[1])
        return remote(
            part.at[layer, h, 1 - core, :, rows], pair.at[layer, h, :, rows],
            pair_send.at[layer, h], pair_recv.at[layer, h], sp, partner,
        )

    def sum_copy(h, layer, dx):
        rows = pl.ds(0, rows_in(h, layer)[1])
        return remote(
            both.at[layer, h, dx, rows], rs_in.at[layer, h, dx, rows],
            rs_send.at[layer, h], rs_recv.at[layer, h], sp, same_core(dx),
        )

    def square_copy(h, layer, d, j):
        return remote(
            ssq.at[layer, h, t], ssq.at[layer, h, t],
            sq_send.at[layer, h], sq_recv.at[layer, h], sp, j,
        )

    def mixed_copy(h, layer, j, recv):
        rows = pl.ds(0, rows_out(h, layer)[1])
        return remote(
            mixed.at[layer, h, rows], mix_in.at[layer, h, t, rows],
            mx_send.at[layer, h], recv.at[layer, h], sp, j,
        )

    def project_in(h, layer):
        start, count = rows_in(h, layer)
        wide = state[start:start + count].astype(F32)
        own_gain = gain[pl.ds(layer, 1), pl.ds(lane0, D // NT)]
        scaled = (wide * own_gain).astype(BF16)
        weights = wi[layer].reshape(P_SIZE, D // NT)
        partial = lax.dot_general(
            scaled, weights, (((1,), (1,)), ((), ())), preferred_element_type=F32
        ).astype(BF16)
        for j in range(NT):
            part[layer, h, j % 2, j // 2, 0:count] = partial[:, j * 128:(j + 1) * 128]
        pair_copy(h, layer).start()
        squares = jnp.sum(wide * wide, axis=1, keepdims=True)
        squares = jnp.broadcast_to(squares, (count, 128))
        squares = jnp.concatenate([squares, jnp.zeros((256 - count, 128), F32)], axis=0)
        ssq[layer, h, t] = squares.T[0:1, :]
        for d in OTHERS:
            square_copy(h, layer, d, peer(d)).start()

    def chip_sum(h, layer, to):
        count = rows_in(h, layer)[1]
        own = part[layer, h, core, to, 0:count].astype(F32)
        return own + pair[layer, h, to, 0:count].astype(F32)

    def combine(h, layer):
        count = rows_in(h, layer)[1]
        landed(pair.at[layer, h, :, pl.ds(0, count)], pair_recv.at[layer, h])
        for dx in (2, 1, 3):
            total = chip_sum(h, layer, (chip + dx) % 4)
            both[layer, h, dx, 0:count] = total.astype(BF16)
            sum_copy(h, layer, dx).start()

    def pool(h, layer, tail):
        count = rows_in(h, layer)[1]
        start, out_count = rows_out(h, layer)
        seven = pl.ds(0, NT - 1)
        landed(ssq.at[layer, h, seven], sq_recv.at[layer, h])
        inv_rms = lax.rsqrt(jnp.sum(ssq[layer, h], axis=0) / D + EPS)
        inv_rms = jnp.broadcast_to(inv_rms, (128, 256)).T[0:count]
        total = chip_sum(h, layer, chip)
        landed(rs_in.at[layer, h, pl.ds(0, 3), pl.ds(0, count)], rs_recv.at[layer, h])
        for dx in (1, 2, 3):
            total = total + rs_in[layer, h, dx, 0:count].astype(F32)
        pool_in = (total * inv_rms).astype(BF16).astype(F32)
        run = pool_in if tail is None else jnp.concatenate([tail, pool_in], axis=0)
        own = run[HALO:]
        picked = None
        for g in range(4):
            run = run + pltpu.roll(run, 1 << g, 0)
            picked = run if g == 0 else jnp.where(group >= g, run, picked)
        means = picked[HALO:] * inverse[start:start + out_count] - own
        own_scale = scale[pl.ds(layer, 1), pl.ds(lane1, 128)]
        mixed[layer, h, 0:out_count] = (means * own_scale).astype(BF16)
        for dx in (2, 1, 3):
            mixed_copy(h, layer, same_core(dx), mx_recv).start()
        mixed_copy(h, layer, partner, px_recv).start()
        mix_in[layer, h, t, 0:out_count] = mixed[layer, h, 0:out_count]
        return pool_in[count - HALO:]

    def relay(h, layer):
        rows = pl.ds(0, rows_out(h, layer)[1])
        landed(mix_in.at[layer, h, pl.ds(0, 3), rows], mx_recv.at[layer, h])
        for dx in (1, 2, 3):
            block = mix_in.at[layer, h, same_core(dx), rows]
            remote(
                block, block, mx_send.at[layer, h], px_recv.at[layer, h], sp, partner
            ).start()

    def project_out(h, layer):
        start, count = rows_out(h, layer)
        landed(mix_in.at[layer, h, pl.ds(0, 4), pl.ds(0, count)], px_recv.at[layer, h])
        pooled = jnp.concatenate(
            [mix_in[layer, h, k, 0:count] for k in range(NT)], axis=1
        )
        branch = jnp.dot(
            pooled, wo[layer].reshape(P_SIZE, D // NT), preferred_element_type=F32
        )
        after = (state[start:start + count].astype(F32) + branch).astype(BF16)
        if layer == LAYERS - 1:
            out_ref[start - AHEAD:start - AHEAD + count] = after
        else:
            state[start:start + count] = after

    project_in(0, 0)
    advance("pre0", 0)
    combine(0, 0)
    project_in(1, 0)
    combine(1, 0)
    for layer in range(LAYERS):
        advance("pool0", layer)
        tail = pool(0, layer, None)
        advance("pool1", layer)
        pool(1, layer, tail)
        advance("pass0", layer)
        relay(0, layer)
        advance("out0", layer)
        project_out(0, layer)
        if layer < LAYERS - 1:
            advance("in0", layer + 1)
            project_in(0, layer + 1)
            advance("pre0", layer + 1)
            combine(0, layer + 1)
        relay(1, layer)
        advance("out1", layer)
        project_out(1, layer)
        if layer < LAYERS - 1:
            project_in(1, layer + 1)
            combine(1, layer + 1)

    def left(blocks, sem):
        remote(blocks, blocks, sem, sem, sp, t).wait_send()

    ahead.wait_send()
    for p in range(2 * LAYERS):
        if p in ROUND:
            left(piece(p).at[pl.ds(0, 15)], z_send.at[p])
            left(piece(p).at[pl.ds(0, 3), 0], y_send.at[p])
        else:
            left(piece(p).at[pl.ds(0, 15), 0], z_send.at[p])
            left(piece(p).at[pl.ds(0, 12)], y_send.at[p])
    seven = pl.ds(0, NT - 1)
    for layer in range(LAYERS):
        for h in (0, 1):
            count, out_count = rows_in(h, layer)[1], rows_out(h, layer)[1]
            left(ssq.at[layer, h, seven], sq_send.at[layer, h])
            left(pair.at[layer, h, :, pl.ds(0, count)], pair_send.at[layer, h])
            left(both.at[layer, h, pl.ds(0, 3), pl.ds(0, count)], rs_send.at[layer, h])
            left(mix_in.at[layer, h, seven, pl.ds(0, out_count)], mx_send.at[layer, h])


def body(inputs, norm_gain, in_weight, pool_scale, out_weight):
    rows, features = inputs.shape
    vmem = pl.BlockSpec(memory_space=pltpu.VMEM)
    hbm = pl.BlockSpec(memory_space=pl.ANY)
    dma = pltpu.SemaphoreType.DMA
    pieces = 2 * LAYERS
    gathered = pltpu.VMEM((LAYERS, NZ, NY, P_SIZE // 64, features), BF16)
    most = AHEAD + SPLIT
    blocks = pltpu.VMEM((LAYERS, 2, NT, most, 128), BF16)
    quarter = pltpu.VMEM((LAYERS, 2, 4, most, 128), BF16)
    return pl.pallas_call(
        kernel,
        out_shape=jax.ShapeDtypeStruct(inputs.shape, inputs.dtype),
        in_specs=[hbm] * 5,
        out_specs=vmem,
        scratch_shapes=[
            gathered, gathered,
            pltpu.VMEM((AHEAD + rows, features), BF16),
            pltpu.VMEM(norm_gain.shape, F32),
            pltpu.VMEM(pool_scale.shape, F32),
            pltpu.VMEM((AHEAD + rows, 128), F32),
            pltpu.VMEM((LAYERS, 2, 2, 4, most, 128), BF16),
            quarter, quarter, quarter,
            pltpu.VMEM((LAYERS, 2, NT, 1, rows), F32),
            pltpu.VMEM((LAYERS, 2, most, 128), BF16),
            blocks,
            dma((pieces,)), dma((pieces, 2)),
            dma((pieces,)), dma((pieces, 4)),
            dma((LAYERS, 2)), dma((LAYERS, 2)),
            dma((LAYERS, 2)), dma((LAYERS, 2)),
            dma((LAYERS, 2)), dma((LAYERS, 2)),
            dma((LAYERS, 2)), dma((LAYERS, 2)), dma((LAYERS, 2)),
            dma((1,)), dma((1,)),
            dma((4,)), dma((2, 8)),
        ],
        compiler_params=pltpu.CompilerParams(
            collective_id=0, has_side_effects=True, vmem_limit_bytes=VMEM_LIMIT
        ),
        name="mixer",
    )(inputs, norm_gain, jnp.swapaxes(in_weight, 1, 2), pool_scale, out_weight)


def solution(mesh):
    placed = (P("sp", "tp"), P(), P(None, "tp", "sp"), P(), P(None, "sp", "tp"))
    return jax.shard_map(body, mesh=mesh, in_specs=placed, out_specs=P("sp", "tp"), check_vma=False)
```

```python
import functools

import jax
import jax.numpy as jnp
from jax import lax
from jax.experimental import pallas as pl
from jax.experimental.pallas import tpu as pltpu
from jax.sharding import PartitionSpec as P

D = 4096
P_SIZE = 1024
LAYERS = 3
EPS = 1e-06
HALO = 16
AHEAD, SPLIT = 48, 128
NZ, NY, NT = 16, 4, 8
MESH = pl.DeviceIdType.MESH
BF16, F32 = jnp.bfloat16, jnp.float32


VMEM_LIMIT = 60 * 1024 * 1024
OTHERS = (4, 5, 2, 3, 6, 7, 1)
RELAYS = ((-6, (2, 1, -1)), (6, (1, -1)), (-2, (2, 1, -1)), (2, (-2, -1, 1)))
FIRST = (2, -6, -2, 6)
LATER = (1, -1, 3, -3, 4, -4, 5, -5, 7, -7, 8)
ROUND = (5,)
PLAN = {
    "start": (
        (0, 0), (5, 0), (1, 0), (0, 1), (5, 1), (2, 0), (1, 1), (0, 2), (5, 2), (3, 0), (0, 3), (2, 1), (1, 2), (4, 0), (5, 3), (0, 4),
    ),
    ("pre0", 0): (
        (1, 3, 1), (2, 2), (3, 1),
    ),
    ("pool0", 0): (
        (1, 3, 0), (5, 4),
    ),
    ("pool1", 0): (
        (5, 5), (4, 1),
    ),
    ("out0", 0): (
        (1, 4), (3, 2), (5, 6),
    ),
    ("in0", 1): (
        (2, 4),
    ),
    ("pre0", 1): (
        (4, 2),
    ),
    ("out1", 0): (
        (5, 7),
    ),
    ("pool0", 1): (
        (3, 3), (5, 8),
    ),
    ("pool1", 1): (
        (4, 3),
    ),
    ("out0", 1): (
        (3, 4), (5, 9),
    ),
    ("in0", 2): (
        (4, 4),
    ),
    ("out1", 1): (
        (5, 10),
    ),
    ("pass0", 0): (
        (2, 3),
    ),
}


def remote(src, dst, send, recv, sp, tp):
    return pltpu.make_async_remote_copy(
        src_ref=src, dst_ref=dst, send_sem=send, recv_sem=recv,
        device_id=(sp, tp), device_id_type=MESH,
    )


def kernel(
    x_ref, gain_ref, win_ref, scale_ref, wout_ref, out_ref,
    wi, wo, state, gain, scale, inverse, part, pair, both, rs_in, ssq, mixed, mix_in,
    z_send, z_recv, y_send, y_recv, rs_send, rs_recv,
    sq_send, sq_recv, mx_send, mx_recv, pair_send, pair_recv, px_recv, h_send, h_recv, own_sem, r_recv,
):
    sp = lax.axis_index("sp")
    t = lax.axis_index("tp")
    z, y = sp // NY, sp % NY

    def at(zz, yy):
        return ((zz + NZ) % NZ) * NY + (yy + NY) % NY

    def peer(d):
        return ((t // 2 + d // 2) % 4) * 2 + (t + d) % 2

    sp_next, sp_prev = (sp + 1) % (NZ * NY), (sp + NZ * NY - 1) % (NZ * NY)

    barrier = pltpu.get_barrier_semaphore()
    greeted = [at(z + o, y) for o in (1, -1, 2, -2, 6, -6)]
    greeted += [at(z, y + 1), at(z, y - 1), sp_next, sp_prev]
    for to in greeted:
        pl.semaphore_signal(barrier, inc=1, device_id=(to, t), device_id_type=MESH)
    for d in OTHERS:
        pl.semaphore_signal(barrier, inc=1, device_id=(sp, peer(d)), device_id_type=MESH)

    own = []
    for layer in range(LAYERS):
        own.append(pltpu.make_async_copy(win_ref.at[layer], wi.at[layer, z, y], own_sem.at[0]))
        own.append(pltpu.make_async_copy(wout_ref.at[layer], wo.at[layer, z, y], own_sem.at[0]))
    own.append(pltpu.make_async_copy(x_ref, state.at[pl.ds(AHEAD, 256)], own_sem.at[1]))
    own.append(pltpu.make_async_copy(gain_ref, gain, own_sem.at[2]))
    own.append(pltpu.make_async_copy(scale_ref, scale, own_sem.at[3]))
    for copy in own:
        copy.start()
    six = wi.at[0, pl.ds(0, 2 * LAYERS), 0]
    pltpu.make_async_copy(six, six, own_sem.at[0]).wait()
    for copy in own[2 * LAYERS:]:
        copy.wait()
    pl.semaphore_wait(barrier, len(greeted) + NT - 1)

    def piece(p):
        return (wo if p % 2 else wi).at[p // 2]

    def line(offset):
        return (z + offset + 2 * NZ) % NZ

    def along_z(p, offset, way, slot):
        block = piece(p).at[line(offset), y]
        remote(block, block, z_send.at[p], z_recv.at[p, slot], at(z + way, y), t).start()

    def along_y(p, offset, from_y, way, slot):
        block = piece(p).at[line(offset), (y + from_y + NY) % NY]
        remote(block, block, y_send.at[p], y_recv.at[p, slot], at(z, y + way), t).start()

    def landed(blocks, sem):
        remote(blocks, blocks, sem, sem, sp, t).wait_recv()

    def stage(p, k):
        if k == 0:
            for way in (6, -6, 2, -2):
                along_z(p, 0, way, 0)
            for way in (1, -1):
                along_y(p, 0, 0, way, 0)
        if k == 1:
            landed(piece(p).at[pl.ds(0, 4), 0], z_recv.at[p, 0])
            for offset, ways in RELAYS:
                for way in ways:
                    along_z(p, offset, way, 1)
            for way in (1, -1):
                for offset in FIRST:
                    along_y(p, offset, 0, way, 0)
        if k == 2:
            landed(piece(p).at[pl.ds(0, 11), 0], z_recv.at[p, 1])
            for way in (1, -1):
                for offset in LATER[:5] if way > 0 else LATER[5:]:
                    along_y(p, offset, 0, way, 1)
            for way in (1, -1):
                for offset in LATER[5:] if way > 0 else LATER[:5]:
                    along_y(p, offset, 0, way, 3)
            landed(piece(p).at[pl.ds(0, 5), pl.ds(0, 2)], y_recv.at[p, 0])
            for offset in (0, 2, -6):
                along_y(p, offset, -1, 1, 2)
            for offset in (-2, 6):
                along_y(p, offset, 1, -1, 2)
        if k == 3:
            landed(piece(p).at[pl.ds(0, 11), 0], y_recv.at[p, 1])
            for offset in LATER[:5]:
                along_y(p, offset, -1, 1, 2)
            for offset in LATER[5:]:
                along_y(p, offset, 1, -1, 2)
        if k == 4:
            landed(piece(p).at[pl.ds(0, 11), 0], y_recv.at[p, 3])
            landed(piece(p).at[:, 0], y_recv.at[p, 2])

    def ring_copy(p, way, step):
        row = piece(p).at[line(-way * step)]
        remote(
            row, row, z_send.at[p], r_recv.at[p - ROUND[0], step], at(z + way, y), t
        ).start()

    def ring_stage(p, k):
        if k == 0:
            for way in (1, -1):
                along_y(p, 0, 0, way, 0)
        if k == 1:
            landed(piece(p).at[pl.ds(0, 2), 0], y_recv.at[p, 0])
            for way in (1, -1):
                half = piece(p).at[z, (y - way + NY) % NY, :, pl.ds(128 + 128 * way, 256)]
                remote(half, half, y_send.at[p], y_recv.at[p, 1], at(z, y + way), t).start()
        if k == 2:
            landed(piece(p).at[0, 0], y_recv.at[p, 1])
        if 3 <= k <= 10:
            landed(piece(p).at[pl.ds(0, 2 if k < 10 else 1)], r_recv.at[p - ROUND[0], k - 3])
        for way, steps in ((1, 8), (-1, 7)):
            if 2 <= k < 2 + steps:
                ring_copy(p, way, k - 2)

    def advance(*where):
        for p, k, *only in PLAN.get(where[0] if len(where) == 1 else where, ()):
            run = functools.partial(ring_stage if p in ROUND else stage, p, k)
            if only:
                pl.when(t % 2 == only[0])(run)
            else:
                run()

    ahead = remote(
        x_ref.at[pl.ds(256 - AHEAD, AHEAD)], state.at[pl.ds(0, AHEAD)],
        h_send.at[0], h_recv.at[0], sp_next, t,
    )
    ahead.start()
    window = jnp.left_shift(jnp.int32(2), t // 2)
    position = sp * 256 - AHEAD + lax.broadcasted_iota(jnp.int32, inverse.shape, 0)
    count = jnp.maximum(jnp.minimum(position + 1, window), 1)
    inverse[...] = 1.0 / count.astype(F32)
    advance("start")
    ahead.wait_recv()
    first = state[0:AHEAD].astype(F32) * (sp > 0).astype(F32)
    state[0:AHEAD] = first.astype(BF16)

    lane0 = pl.multiple_of(t * (D // NT), 128)
    lane1 = pl.multiple_of(t * 128, 128)
    group = t // 2

    def rows_in(h, layer):
        return (HALO * layer, AHEAD + SPLIT - HALO * layer) if h == 0 else (AHEAD + SPLIT, 256 - SPLIT)

    def rows_out(h, layer):
        start, count = rows_in(h, layer)
        return (start, count) if h else (start + HALO, count - HALO)

    chip, core = t // 2, t % 2
    partner = chip * 2 + 1 - core

    def same_core(dx):
        return ((chip + dx) % 4) * 2 + core

    def pair_copy(h, layer):
        rows = pl.ds(0, rows_in(h, layer)[1])
        return remote(
            part.at[layer, h, 1 - core, :, rows], pair.at[layer, h, :, rows],
            pair_send.at[layer, h], pair_recv.at[layer, h], sp, partner,
        )

    def sum_copy(h, layer, dx):
        rows = pl.ds(0, rows_in(h, layer)[1])
        return remote(
            both.at[layer, h, dx, rows], rs_in.at[layer, h, dx, rows],
            rs_send.at[layer, h], rs_recv.at[layer, h], sp, same_core(dx),
        )

    def square_copy(h, layer, d, j):
        return remote(
            ssq.at[layer, h, t], ssq.at[layer, h, t],
            sq_send.at[layer, h], sq_recv.at[layer, h], sp, j,
        )

    def mixed_copy(h, layer, j, recv):
        rows = pl.ds(0, rows_out(h, layer)[1])
        return remote(
            mixed.at[layer, h, rows], mix_in.at[layer, h, t, rows],
            mx_send.at[layer, h], recv.at[layer, h], sp, j,
        )

    def project_in(h, layer):
        start, count = rows_in(h, layer)
        wide = state[start:start + count].astype(F32)
        own_gain = gain[pl.ds(layer, 1), pl.ds(lane0, D // NT)]
        scaled = (wide * own_gain).astype(BF16)
        weights = wi[layer].reshape(P_SIZE, D // NT)
        partial = lax.dot_general(
            scaled, weights, (((1,), (1,)), ((), ())), preferred_element_type=F32
        ).astype(BF16)
        for j in range(NT):
            part[layer, h, j % 2, j // 2, 0:count] = partial[:, j * 128:(j + 1) * 128]
        pair_copy(h, layer).start()
        squares = jnp.sum(wide * wide, axis=1, keepdims=True)
        squares = jnp.broadcast_to(squares, (count, 128))
        squares = jnp.concatenate([squares, jnp.zeros((256 - count, 128), F32)], axis=0)
        ssq[layer, h, t] = squares.T[0:1, :]
        for d in OTHERS:
            square_copy(h, layer, d, peer(d)).start()

    def chip_sum(h, layer, to):
        count = rows_in(h, layer)[1]
        own = part[layer, h, core, to, 0:count].astype(F32)
        return own + pair[layer, h, to, 0:count].astype(F32)

    def combine(h, layer):
        count = rows_in(h, layer)[1]
        landed(pair.at[layer, h, :, pl.ds(0, count)], pair_recv.at[layer, h])
        for dx in (2, 1, 3):
            total = chip_sum(h, layer, (chip + dx) % 4)
            both[layer, h, dx, 0:count] = total.astype(BF16)
            sum_copy(h, layer, dx).start()

    def pool(h, layer, tail):
        count = rows_in(h, layer)[1]
        start, out_count = rows_out(h, layer)
        seven = pl.ds(0, NT - 1)
        landed(ssq.at[layer, h, seven], sq_recv.at[layer, h])
        inv_rms = lax.rsqrt(jnp.sum(ssq[layer, h], axis=0) / D + EPS)
        inv_rms = jnp.broadcast_to(inv_rms, (128, 256)).T[0:count]
        total = chip_sum(h, layer, chip)
        landed(rs_in.at[layer, h, pl.ds(0, 3), pl.ds(0, count)], rs_recv.at[layer, h])
        for dx in (1, 2, 3):
            total = total + rs_in[layer, h, dx, 0:count].astype(F32)
        pool_in = (total * inv_rms).astype(BF16).astype(F32)
        run = pool_in if tail is None else jnp.concatenate([tail, pool_in], axis=0)
        own = run[HALO:]
        picked = None
        for g in range(4):
            run = run + pltpu.roll(run, 1 << g, 0)
            picked = run if g == 0 else jnp.where(group >= g, run, picked)
        means = picked[HALO:] * inverse[start:start + out_count] - own
        own_scale = scale[pl.ds(layer, 1), pl.ds(lane1, 128)]
        mixed[layer, h, 0:out_count] = (means * own_scale).astype(BF16)
        for dx in (2, 1, 3):
            mixed_copy(h, layer, same_core(dx), mx_recv).start()
        mixed_copy(h, layer, partner, px_recv).start()
        mix_in[layer, h, t, 0:out_count] = mixed[layer, h, 0:out_count]
        return pool_in[count - HALO:]

    def relay(h, layer):
        rows = pl.ds(0, rows_out(h, layer)[1])
        landed(mix_in.at[layer, h, pl.ds(0, 3), rows], mx_recv.at[layer, h])
        for dx in (1, 2, 3):
            block = mix_in.at[layer, h, same_core(dx), rows]
            remote(
                block, block, mx_send.at[layer, h], px_recv.at[layer, h], sp, partner
            ).start()

    def project_out(h, layer):
        start, count = rows_out(h, layer)
        landed(mix_in.at[layer, h, pl.ds(0, 4), pl.ds(0, count)], px_recv.at[layer, h])
        pooled = jnp.concatenate(
            [mix_in[layer, h, k, 0:count] for k in range(NT)], axis=1
        )
        branch = jnp.dot(
            pooled, wo[layer].reshape(P_SIZE, D // NT), preferred_element_type=F32
        )
        after = (state[start:start + count].astype(F32) + branch).astype(BF16)
        if layer == LAYERS - 1:
            out_ref[start - AHEAD:start - AHEAD + count] = after
        else:
            state[start:start + count] = after

    project_in(0, 0)
    advance("pre0", 0)
    combine(0, 0)
    project_in(1, 0)
    combine(1, 0)
    for layer in range(LAYERS):
        advance("pool0", layer)
        tail = pool(0, layer, None)
        advance("pool1", layer)
        pool(1, layer, tail)
        advance("pass0", layer)
        relay(0, layer)
        advance("out0", layer)
        project_out(0, layer)
        if layer < LAYERS - 1:
            advance("in0", layer + 1)
            project_in(0, layer + 1)
            advance("pre0", layer + 1)
        relay(1, layer)
        if layer < LAYERS - 1:
            combine(0, layer + 1)
        advance("out1", layer)
        project_out(1, layer)
        if layer < LAYERS - 1:
            project_in(1, layer + 1)
            combine(1, layer + 1)

    def left(blocks, sem):
        remote(blocks, blocks, sem, sem, sp, t).wait_send()

    ahead.wait_send()
    for p in range(2 * LAYERS):
        if p in ROUND:
            left(piece(p).at[pl.ds(0, 15)], z_send.at[p])
            left(piece(p).at[pl.ds(0, 3), 0], y_send.at[p])
        else:
            left(piece(p).at[pl.ds(0, 15), 0], z_send.at[p])
            left(piece(p).at[pl.ds(0, 12)], y_send.at[p])
    seven = pl.ds(0, NT - 1)
    for layer in range(LAYERS):
        for h in (0, 1):
            count, out_count = rows_in(h, layer)[1], rows_out(h, layer)[1]
            left(ssq.at[layer, h, seven], sq_send.at[layer, h])
            left(pair.at[layer, h, :, pl.ds(0, count)], pair_send.at[layer, h])
            left(both.at[layer, h, pl.ds(0, 3), pl.ds(0, count)], rs_send.at[layer, h])
            left(mix_in.at[layer, h, seven, pl.ds(0, out_count)], mx_send.at[layer, h])


def body(inputs, norm_gain, in_weight, pool_scale, out_weight):
    rows, features = inputs.shape
    vmem = pl.BlockSpec(memory_space=pltpu.VMEM)
    hbm = pl.BlockSpec(memory_space=pl.ANY)
    dma = pltpu.SemaphoreType.DMA
    pieces = 2 * LAYERS
    gathered = pltpu.VMEM((LAYERS, NZ, NY, P_SIZE // 64, features), BF16)
    most = AHEAD + SPLIT
    blocks = pltpu.VMEM((LAYERS, 2, NT, most, 128), BF16)
    quarter = pltpu.VMEM((LAYERS, 2, 4, most, 128), BF16)
    return pl.pallas_call(
        kernel,
        out_shape=jax.ShapeDtypeStruct(inputs.shape, inputs.dtype),
        in_specs=[hbm] * 5,
        out_specs=vmem,
        scratch_shapes=[
            gathered, gathered,
            pltpu.VMEM((AHEAD + rows, features), BF16),
            pltpu.VMEM(norm_gain.shape, F32),
            pltpu.VMEM(pool_scale.shape, F32),
            pltpu.VMEM((AHEAD + rows, 128), F32),
            pltpu.VMEM((LAYERS, 2, 2, 4, most, 128), BF16),
            quarter, quarter, quarter,
            pltpu.VMEM((LAYERS, 2, NT, 1, rows), F32),
            pltpu.VMEM((LAYERS, 2, most, 128), BF16),
            blocks,
            dma((pieces,)), dma((pieces, 2)),
            dma((pieces,)), dma((pieces, 4)),
            dma((LAYERS, 2)), dma((LAYERS, 2)),
            dma((LAYERS, 2)), dma((LAYERS, 2)),
            dma((LAYERS, 2)), dma((LAYERS, 2)),
            dma((LAYERS, 2)), dma((LAYERS, 2)), dma((LAYERS, 2)),
            dma((1,)), dma((1,)),
            dma((4,)), dma((2, 8)),
        ],
        compiler_params=pltpu.CompilerParams(
            collective_id=0, has_side_effects=True, vmem_limit_bytes=VMEM_LIMIT
        ),
        name="mixer",
    )(inputs, norm_gain, jnp.swapaxes(in_weight, 1, 2), pool_scale, out_weight)


def solution(mesh):
    placed = (P("sp", "tp"), P(), P(None, "tp", "sp"), P(), P(None, "sp", "tp"))
    return jax.shard_map(body, mesh=mesh, in_specs=placed, out_specs=P("sp", "tp"), check_vma=False)
```
